256 devices in a mesh: grp: 4 (over y, x), ep: 32 (over z), tp: 2 (over core).
Axes of the slice: x: 2, y: 2, z: 32, core: 2. Of those that a mesh axis runs over, the one named last changes fastest.
The devices are a block of a 4x16x32 slice.
Arguments:
- tokens: bfloat16 [4096, 2048], P(('grp', 'ep'), 'tp'), parts along dimension 0, may hold values from -6 to 6
- routes: int32 [4096, 4], P(('grp', 'ep')), parts along dimension 0, may hold values from 0 to 31, all different within a row; in each aligned block of 32 rows (0 to 31, 32 to 63, ...) at most 6 rows name the same one
- gate_logits: float32 [4096, 4], P(('grp', 'ep')), parts along dimension 0, may hold values from -6 to 6
- norm_gain: float32 [2048], P('tp'), may hold values from 0.1 to 1.9
- norm_shift: float32 [2048], P('tp'), may hold values from -3 to 3
- gate_weight: bfloat16 [32, 2048, 1024], P('ep', None, 'tp'), may hold values from -0.5 to 0.5
- up_weight: bfloat16 [32, 2048, 1024], P('ep', None, 'tp'), may hold values from -0.5 to 0.5
- down_weight: bfloat16 [32, 1024, 2048], P('ep', 'tp'), may hold values from -0.0234375 to 0.0234375
Outputs:
- mixed: bfloat16 [4096, 2048], P(('grp', 'ep'), 'tp'), parts along dimension 0
The draws below stay inside these ranges and needn't reach their ends.
There are 4 independent parts, one for each index of `grp`. The reference program is written for one: setup_inputs(seed, part) draws one part's arguments, and reference() takes and returns one part's arrays. A program takes and returns all parts, laid end to end along the dimension named above; an argument that names none is the same for every part. Nothing has to cross between parts.
Inputs may be any that keep to these rules, and one draw needn't show every extreme that they name: `routes`: each row names 4 different experts. Within the 32 rows of one index of ep no expert is named more than 6 times, a bound that some blocks reach.
All inputs are finite; a program needn't handle non-finite values.
Results may differ from the reference program's by a relative error of at most 0.012.
Values may be sent and summed in bfloat16 or wider, within the bound.
No kernel may reach another device: no remote copies, remote signals or barrier semaphores. Data moves between devices by JAX's collectives and lax.ppermute only.
A program may use at most 64 MiB of HBM per device.

```python
import math
import jax
import jax.numpy as jnp
import numpy as np
from jax import lax

D = 2048
FF = 1024
TOP_K = 4
TOK_DEV = 32
EXPERTS = 32
CAP = 6
SLOTS = 192
TOKENS = 1024
N_EP = 32
N_TP = 2


def shard_levels(own_key, dims, pieces, least, top_value):
    factor_of, own = 1.0, jax.random.fold_in(own_key, 6)
    for position, blocks in pieces:
        heights = jnp.exp(jax.random.uniform(jax.random.fold_in(own, position), (blocks,), jnp.float32, least / len(pieces), top_value / len(pieces)))
        factor_of = factor_of * jnp.repeat(heights, dims[position] // blocks).reshape([-1 if axis == position else 1 for axis in range(len(dims))])
    return factor_of


def shared_out(stream_key, own, number, rows, amount, top, limit, lean):
    ranking = jax.random.permutation(stream_key, amount)
    crowded, common = shares(amount, rows * top, limit, lean, True), shares(amount, rows * top, limit, lean, False)
    places = jnp.arange(amount)

    def named(sizes, rotation):
        used = int((sizes > 0).sum())
        fixed = max(1, used // 4)
        passed = fixed + (places - fixed + rotation * (used - fixed)) % max(1, amount - fixed)
        return jnp.zeros((amount,), jnp.int32).at[ranking[jnp.where(places < fixed, places, passed)]].set(jnp.asarray(sizes, jnp.int32))

    sizes = jnp.where(number % 4 == 0, named(crowded, number // 4), named(common, number - number // 4 - 1))
    mixed = jax.random.permutation(jax.random.fold_in(own, 3), amount)
    giver, sink = mixed[0:amount // 2 * 2:2], mixed[1:amount // 2 * 2:2]
    margin = jnp.minimum(sizes[giver] - 1, limit - sizes[sink]) // 2
    margin = jnp.where((giver == ranking[0]) | (sink == ranking[0]) | (sizes[sink] == 0), 0, jnp.maximum(margin, 0))
    passed = jax.random.randint(jax.random.fold_in(own, 4), (amount // 2,), 0, 1 << 20) % (margin + 1)
    sizes = sizes.at[giver].add(-passed).at[sink].add(passed)
    labels = jnp.searchsorted(jnp.cumsum(sizes), jnp.arange(rows * top), side="right").astype(jnp.int32)
    table = labels.reshape(top, rows).T
    table = table[jax.random.permutation(jax.random.fold_in(own, 1), rows)]
    rotation = jax.random.randint(jax.random.fold_in(own, 2), (rows, 1), 0, top)
    return jnp.take_along_axis(table, (jnp.arange(top)[None, :] + rotation) % top, axis=1)


def shares(amount, total, reach, slope, full):
    portions = [(1 << 20) // math.isqrt(grade ** slope) + 1 for grade in range(1, amount + 1)]
    largest = reach if full else min(reach, max(-(-total // amount), total * portions[0] // sum(portions)))
    least = 1 if total - largest >= amount - 1 else 0
    given, spare = [largest] + [least] * (amount - 1), total - largest - least * (amount - 1)
    while spare > 0:
        candidates = [i for i in range(1, amount) if given[i] < largest] or [i for i in range(1, amount) if given[i] < reach]
        whole, remaining = sum([portions[i] for i in candidates]), spare
        for i in candidates:
            more = min(reach - given[i], max(1, remaining * portions[i] // whole), spare)
            given[i] = given[i] + more
            spare = spare - more
    return np.array(given)


def gaussian(own_key, extent, scale, most, cuts=(), kind=jnp.bfloat16):
    entries = scale * jax.random.normal(own_key, extent, jnp.float32)
    if cuts:
        entries = entries * shard_levels(own_key, extent, cuts, -0.22, 0.18)
    return jnp.clip(entries, -most, most).astype(kind)


def setup_inputs(seed: int = 0, part: int = 0) -> dict:
    key_list = jax.random.split(jax.random.key(seed), 9)
    part_splits = jax.random.split(jax.random.fold_in(key_list[8], part), 9)
    tokens = gaussian(part_splits[0], (TOKENS, D), 1.0, 6.0, ((0, 32), (1, 2)))
    routes_keys = jax.random.split(jax.random.fold_in(part_splits[1], 1), TOKENS // TOK_DEV)
    routes_turns = jax.random.permutation(jax.random.fold_in(part_splits[1], 3), TOKENS // TOK_DEV)
    routes = jax.vmap(lambda own, number: shared_out(jax.random.fold_in(part_splits[1], 2), own, number, TOK_DEV, EXPERTS, TOP_K, CAP, 2))(routes_keys, routes_turns).reshape((TOKENS, TOP_K))
    gate_logits = gaussian(part_splits[2], (TOKENS, TOP_K), 1.5, 6.0, ((0, 32),), jnp.float32)
    norm_gain = jnp.clip(1.0 + 0.18 * jax.random.normal(key_list[3], (D,), jnp.float32), 0.1, 1.9)
    norm_shift = gaussian(key_list[4], (D,), 0.5, 3.0, ((0, 2),), jnp.float32)
    gate_weight = gaussian(key_list[5], (EXPERTS, D, FF), (D // 16) ** -0.5, 0.5, ((0, 32), (2, 2)))
    up_weight = gaussian(key_list[6], (EXPERTS, D, FF), (D // 16) ** -0.5, 0.5, ((0, 32), (2, 2)))
    down_weight = gaussian(key_list[7], (EXPERTS, FF, D), (FF * 64) ** -0.5, 0.0234375, ((0, 32), (1, 2)))
    return {"tokens": tokens, "routes": routes, "gate_logits": gate_logits, "norm_gain": norm_gain, "norm_shift": norm_shift, "gate_weight": gate_weight, "up_weight": up_weight, "down_weight": down_weight}


norm_eps = 1e-05
clamp_limit = 7.0
sigmoid_slope = 1.702

def one_expert(operands):
    row_block, gate_mat, up_mat, down_mat = operands
    gate_pre = jnp.dot(row_block, gate_mat, preferred_element_type=jnp.float32)
    up_pre = jnp.dot(row_block, up_mat, preferred_element_type=jnp.float32)
    gate_cut = jnp.minimum(gate_pre, clamp_limit)
    up_cut = jnp.clip(up_pre, -clamp_limit, clamp_limit)
    hidden = ((up_cut + 1.0) * gate_cut * jax.nn.sigmoid(sigmoid_slope * gate_cut)).astype(jnp.bfloat16)
    portion_width = FF // N_TP
    running = jnp.zeros((row_block.shape[0], D), jnp.float32)
    for portion in range(N_TP):
        lower = portion * portion_width
        partial_out = jnp.dot(hidden[:, lower:lower + portion_width], down_mat[lower:lower + portion_width], preferred_element_type=jnp.float32).astype(jnp.bfloat16)
        partial_out = lax.optimization_barrier(partial_out)
        running = running + partial_out.astype(jnp.float32)
    return running.astype(jnp.bfloat16)

def reference(tokens, routes, gate_logits, norm_gain, norm_shift, gate_weight, up_weight, down_weight):
    floats = tokens.astype(jnp.float32)
    average = lax.optimization_barrier(jnp.sum(floats, axis=1)) / D
    variance = lax.optimization_barrier(jnp.sum(floats * floats, axis=1)) / D - average * average
    normed = ((floats - average[:, None]) * lax.rsqrt(variance[:, None] + norm_eps) * norm_gain + norm_shift).astype(jnp.bfloat16)
    exp_logits = jnp.exp(gate_logits)
    weights = exp_logits / lax.optimization_barrier(jnp.sum(exp_logits, axis=1, keepdims=True))
    flat_experts = routes.reshape(N_EP, TOK_DEV * TOP_K)
    onehot = (flat_experts[:, :, None] == jnp.arange(EXPERTS, dtype=jnp.int32)[None, None, :]).astype(jnp.int32)
    rank_in = lax.optimization_barrier(jnp.sum((jnp.cumsum(onehot, axis=1) - onehot) * onehot, axis=2))
    source = jnp.arange(N_EP, dtype=jnp.int32)[:, None]
    slot_index = (flat_experts * SLOTS + source * CAP + rank_in).reshape(TOKENS * TOP_K).astype(jnp.int32)
    token_index = jnp.arange(TOKENS * TOP_K, dtype=jnp.int32) // TOP_K
    slot_token = jnp.full((EXPERTS * SLOTS,), TOKENS, jnp.int32).at[slot_index].set(token_index)
    padded = jnp.concatenate([normed, jnp.zeros((1, D), jnp.bfloat16)], axis=0)
    row_blocks = padded[slot_token].reshape(EXPERTS, SLOTS, D)
    expert_out = lax.map(one_expert, (row_blocks, gate_weight, up_weight, down_weight)).reshape(EXPERTS * SLOTS, D)
    picked = expert_out[slot_index].astype(jnp.float32).reshape(TOKENS, TOP_K, D)
    return lax.optimization_barrier(jnp.sum(picked * weights[:, :, None], axis=1)).astype(jnp.bfloat16)
```

```python
import jax
import jax.numpy as jnp
from jax import lax
from jax.sharding import PartitionSpec as P

norm_eps = 1e-05
clamp_limit = 7.0
sigmoid_slope = 1.702
lanes = 128


def swap_tp(x):
    return lax.ppermute(x, "tp", [(0, 1), (1, 0)])


def exchange(x):
    return lax.all_to_all(x, "ep", split_axis=0, concat_axis=0, tiled=True)


def normalised(tokens, norm_gain, norm_shift):
    floats = tokens.astype(jnp.float32)
    own = jnp.stack([jnp.sum(floats, axis=1), jnp.sum(floats * floats, axis=1)])
    sums = own + swap_tp(own)
    full_width = tokens.shape[1] * lax.axis_size("tp")
    average = sums[0] / full_width
    variance = sums[1] / full_width - average * average
    return (
        (floats - average[:, None]) * lax.rsqrt(variance[:, None] + norm_eps) * norm_gain
        + norm_shift
    ).astype(jnp.bfloat16)


def expert_half(rows, gate_weight, up_weight, down_weight):
    gate_pre = jnp.dot(rows, gate_weight[0], preferred_element_type=jnp.float32)
    up_pre = jnp.dot(rows, up_weight[0], preferred_element_type=jnp.float32)
    gate_cut = jnp.minimum(gate_pre, clamp_limit)
    up_cut = jnp.clip(up_pre, -clamp_limit, clamp_limit)
    hidden = ((up_cut + 1.0) * gate_cut * jax.nn.sigmoid(sigmoid_slope * gate_cut)).astype(
        jnp.bfloat16
    )
    return jnp.dot(hidden, down_weight[0], preferred_element_type=jnp.float32).astype(jnp.bfloat16)


def body(tokens, routes, gate_logits, norm_gain, norm_shift, gate_weight, up_weight, down_weight):
    experts = lax.axis_size("ep")
    rows, top_count = routes.shape
    width = tokens.shape[1]
    capacity = rows * top_count // experts + 2
    half = lax.axis_index("tp")
    blocks = width // lanes
    slots = experts * capacity

    normed = normalised(tokens, norm_gain, norm_shift)
    exp_logits = jnp.exp(gate_logits)
    weights = exp_logits / jnp.sum(exp_logits, axis=1, keepdims=True)
    match = routes[:, :, None] == jnp.arange(experts, dtype=jnp.int32)[None, None, :]
    chosen = jnp.any(match, axis=1)
    weight_of = jnp.sum(jnp.where(match, weights[:, :, None], 0.0), axis=1)
    before = (jnp.arange(rows)[:, None] > jnp.arange(rows)[None, :]).astype(jnp.bfloat16)
    rank = jnp.dot(before, chosen.astype(jnp.bfloat16), preferred_element_type=jnp.float32)
    rank = jnp.where(chosen, rank, -1.0)
    places = jnp.arange(capacity, dtype=jnp.float32)
    taken = rank[:, :, None] == places[None, None, :]
    pick = taken.reshape(rows, slots).astype(jnp.bfloat16)
    packed = lax.dot_general(
        pick, normed, (((0,), (0,)), ((), ())), preferred_element_type=jnp.float32
    ).astype(jnp.bfloat16)
    arrived = exchange(packed.reshape(experts, capacity * blocks, lanes))
    other = swap_tp(arrived)
    own_rows = arrived.reshape(slots, width)
    other_rows = other.reshape(slots, width)
    first = jnp.where(half == 0, own_rows, other_rows)
    second = jnp.where(half == 0, other_rows, own_rows)
    partial_out = expert_half(
        jnp.concatenate([first, second], axis=1), gate_weight, up_weight, down_weight
    )
    low, high = (partial_out[:, :width], partial_out[:, width:])
    kept = jnp.where(half == 0, low, high).reshape(experts, capacity * blocks, lanes)
    given = jnp.where(half == 0, high, low).reshape(experts, capacity * blocks, lanes)
    got = swap_tp(given)
    answered = (kept.astype(jnp.float32) + got.astype(jnp.float32)).astype(jnp.bfloat16)
    returned = exchange(answered).reshape(slots, width)
    blend = jnp.where(taken, weight_of[:, :, None], 0.0).reshape(rows, slots)
    blend_high = blend.astype(jnp.bfloat16)
    blend_low = (blend - blend_high.astype(jnp.float32)).astype(jnp.bfloat16)
    mixed = jnp.dot(blend_high, returned, preferred_element_type=jnp.float32) + jnp.dot(
        blend_low, returned, preferred_element_type=jnp.float32
    )
    return mixed.astype(jnp.bfloat16)


def solution(mesh):
    placed = (
        P(("grp", "ep"), "tp"),
        P(("grp", "ep"), None),
        P(("grp", "ep"), None),
        P("tp"),
        P("tp"),
        P("ep", None, "tp"),
        P("ep", None, "tp"),
        P("ep", "tp", None),
    )
    return jax.shard_map(
        body, mesh=mesh, in_specs=placed, out_specs=P(("grp", "ep"), "tp"), check_vma=False
    )
```

```python
import functools

import jax
import jax.numpy as jnp
from jax import lax
from jax.experimental import pallas as pl
from jax.experimental.pallas import tpu as pltpu
from jax.sharding import PartitionSpec as P

norm_eps = 1e-05
clamp_limit = 7.0
sigmoid_slope = 1.702
lanes = 128


def swap_tp(x):
    return lax.ppermute(x, "tp", [(0, 1), (1, 0)])


def exchange(x):
    return lax.all_to_all(x, "ep", split_axis=0, concat_axis=0, tiled=True)


def in_hbm(x):
    return pltpu.with_memory_space_constraint(x, pltpu.HBM)


def load_kernel(tokens_hbm, routes_hbm, logits_hbm, gain_hbm, shift_hbm, gate_hbm, sums_ref, tokens_ref, routes_ref, logits_ref, gain_ref, shift_ref, gate_ref, sems):
    pairs = (
        (tokens_hbm, tokens_ref),
        (routes_hbm, routes_ref),
        (logits_hbm, logits_ref),
        (gain_hbm, gain_ref),
        (shift_hbm, shift_ref),
        (gate_hbm, gate_ref),
    )
    copies = [pltpu.make_async_copy(*pair, sems.at[i]) for i, pair in enumerate(pairs)]
    for copy in copies:
        copy.start()
    copies[0].wait()
    rows, width = tokens_ref.shape
    total = jnp.zeros((rows, lanes), jnp.float32)
    squares = jnp.zeros((rows, lanes), jnp.float32)
    for j in range(width // lanes):
        part = tokens_ref[:, j * lanes : (j + 1) * lanes].astype(jnp.float32)
        total = total + part
        squares = squares + part * part
    sums_ref[:rows, :] = total
    sums_ref[rows:, :] = squares
    for copy in copies[1:]:
        copy.wait()


def plan_kernel(capacity, routes_ref, logits_ref, up_hbm, pick_ref, high_ref, low_ref, up_ref, sem):
    copy = pltpu.make_async_copy(up_hbm, up_ref, sem)
    copy.start()
    top_count, rows = routes_ref.shape
    slots = pick_ref.shape[0]
    experts = slots // capacity
    exp_logits = jnp.exp(logits_ref[...])
    weights = exp_logits / jnp.sum(exp_logits, axis=0, keepdims=True)
    expert_id = lax.broadcasted_iota(jnp.int32, (experts, rows), 0)
    chosen = jnp.zeros((experts, rows), jnp.float32)
    weight_of = jnp.zeros((experts, rows), jnp.float32)
    for k in range(top_count):
        match = routes_ref[k : k + 1, :] == expert_id
        chosen = jnp.where(match, 1.0, chosen)
        weight_of = jnp.where(match, weights[k : k + 1, :], weight_of)
    earlier = lax.broadcasted_iota(jnp.int32, (rows, rows), 0) < lax.broadcasted_iota(
        jnp.int32, (rows, rows), 1
    )
    rank = jnp.dot(
        chosen.astype(jnp.bfloat16),
        jnp.where(earlier, 1.0, 0.0).astype(jnp.bfloat16),
        preferred_element_type=jnp.float32,
    )
    slot_of = jnp.where(
        chosen > 0.0, rank + (expert_id * capacity).astype(jnp.float32), -1.0
    ).astype(jnp.bfloat16)
    slot_id = lax.broadcasted_iota(jnp.int32, (slots, experts), 0)
    first = lax.broadcasted_iota(jnp.int32, (slots, experts), 1) * capacity
    spread = jnp.where((slot_id >= first) & (slot_id < first + capacity), 1.0, 0.0).astype(
        jnp.bfloat16
    )

    def to_slots(x):
        return jnp.dot(spread, x, preferred_element_type=jnp.float32)

    taken = to_slots(slot_of) == lax.broadcasted_iota(jnp.int32, (slots, rows), 0).astype(jnp.float32)
    high = weight_of.astype(jnp.bfloat16)
    low = (weight_of - high.astype(jnp.float32)).astype(jnp.bfloat16)
    pick_ref[...] = jnp.where(taken, 1.0, 0.0).astype(jnp.bfloat16)
    high_ref[...] = jnp.where(taken, to_slots(high), 0.0).astype(jnp.bfloat16)
    low_ref[...] = jnp.where(taken, to_slots(low), 0.0).astype(jnp.bfloat16)
    copy.wait()


def pack_kernel(full_width, tokens_ref, own_ref, other_ref, gain_ref, shift_ref, pick_ref, down_hbm, packed_ref, down_ref, wide, sem):
    copy = pltpu.make_async_copy(down_hbm, down_ref, sem)
    copy.start()
    rows, width = tokens_ref.shape
    slots = pick_ref.shape[0]
    blocks = width // lanes
    sums = jnp.sum(own_ref[...] + other_ref[...], axis=1, keepdims=True)
    average = sums[:rows, :] / full_width
    variance = sums[rows:, :] / full_width - average * average
    inverse = lax.rsqrt(variance + norm_eps)
    normed = [
        (
            (tokens_ref[:, j * lanes : (j + 1) * lanes].astype(jnp.float32) - average)
            * inverse
            * gain_ref[j : j + 1, :]
            + shift_ref[j : j + 1, :]
        ).astype(jnp.bfloat16)
        for j in range(blocks)
    ]
    packed = jnp.dot(
        pick_ref[...], jnp.concatenate(normed, axis=1), preferred_element_type=jnp.float32
    )
    for j in range(blocks):
        wide[pl.ds(j, slots, stride=blocks), :] = packed[:, j * lanes : (j + 1) * lanes]
    packed_ref[...] = wide[...].astype(jnp.bfloat16)
    copy.wait()


def in_kernel(name, kernel, outs, scratch=(), kinds=None):
    vmem = pl.BlockSpec(memory_space=pltpu.VMEM)
    return pl.pallas_call(
        kernel,
        out_shape=tuple(jax.ShapeDtypeStruct(shape, dtype) for shape, dtype in outs),
        in_specs=[pl.BlockSpec(memory_space=kind) for kind in kinds],
        out_specs=tuple(vmem for _ in outs),
        scratch_shapes=list(scratch),
        compiler_params=pltpu.CompilerParams(vmem_limit_bytes=16 << 20),
        name=name,
    )


def expert_kernel(own_ref, other_ref, gate_ref, up_ref, down_ref, kept_ref, given_ref, wide, rows_own, rows_other, out_wide):
    slots, width = rows_own.shape
    blocks = width // lanes
    half = lax.axis_index("tp")
    for source, target in ((own_ref, rows_own), (other_ref, rows_other)):
        wide[...] = source[...].astype(jnp.float32)
        for j in range(blocks):
            target[:, j * lanes : (j + 1) * lanes] = wide[pl.ds(j, slots, stride=blocks), :].astype(
                jnp.bfloat16
            )
    here = pl.multiple_of(half * width, width)
    there = pl.multiple_of((1 - half) * width, width)

    def project(weight_ref):
        return jnp.dot(
            rows_own[...], weight_ref[0, pl.ds(here, width), :], preferred_element_type=jnp.float32
        ) + jnp.dot(
            rows_other[...], weight_ref[0, pl.ds(there, width), :], preferred_element_type=jnp.float32
        )

    gate_cut = jnp.minimum(project(gate_ref), clamp_limit)
    up_cut = jnp.clip(project(up_ref), -clamp_limit, clamp_limit)
    hidden = ((up_cut + 1.0) * gate_cut * jax.nn.sigmoid(sigmoid_slope * gate_cut)).astype(
        jnp.bfloat16
    )
    for side in range(2):
        part = jnp.dot(
            hidden, down_ref[0, :, side * width : (side + 1) * width], preferred_element_type=jnp.float32
        )
        base = jnp.where(half == side, 0, slots * blocks)
        for j in range(blocks):
            out_wide[pl.ds(base + j, slots, stride=blocks), :] = part[:, j * lanes : (j + 1) * lanes]
    kept_ref[...] = out_wide[: slots * blocks, :].astype(jnp.bfloat16)
    given_ref[...] = out_wide[slots * blocks :, :].astype(jnp.bfloat16)


def body(tokens, routes, gate_logits, norm_gain, norm_shift, gate_weight, up_weight, down_weight):
    experts = lax.axis_size("ep")
    rows, top_count = routes.shape
    width = tokens.shape[1]
    full_width = width * lax.axis_size("tp")
    capacity = rows * top_count // experts + 2
    blocks = width // lanes
    slots = experts * capacity
    wire = (experts, capacity * blocks, lanes)
    tiles = (slots * blocks, lanes)
    bf16, f32 = jnp.bfloat16, jnp.float32
    vmem = pltpu.VMEM

    inputs = (tokens, routes.T, gate_logits.T, norm_gain.reshape(blocks, lanes), norm_shift.reshape(blocks, lanes), gate_weight)
    sums, tokens, routes, gate_logits, norm_gain, norm_shift, gate_weight = in_kernel(
        "load",
        load_kernel,
        [((2 * rows, lanes), f32)] + [(x.shape, x.dtype) for x in inputs],
        scratch=[pltpu.SemaphoreType.DMA((len(inputs),))],
        kinds=[pltpu.HBM] * len(inputs),
    )(*(in_hbm(x) for x in inputs))
    other_sums = swap_tp(sums)
    pick, high, low, up_weight = in_kernel(
        "plan",
        functools.partial(plan_kernel, capacity),
        [((slots, rows), bf16)] * 3 + [(up_weight.shape, bf16)],
        scratch=[pltpu.SemaphoreType.DMA(())],
        kinds=[vmem] * 2 + [pltpu.HBM],
    )(routes, gate_logits, in_hbm(up_weight))
    packed, down_weight = in_kernel(
        "pack",
        functools.partial(pack_kernel, full_width),
        [(tiles, bf16), (down_weight.shape, bf16)],
        scratch=[pltpu.VMEM(tiles, f32), pltpu.SemaphoreType.DMA(())],
        kinds=[vmem] * 6 + [pltpu.HBM],
    )(tokens, sums, other_sums, norm_gain, norm_shift, pick, in_hbm(down_weight))
    arrived = exchange(packed.reshape(wire)).reshape(tiles)
    other = swap_tp(arrived)
    kept, given = in_kernel(
        "expert",
        expert_kernel,
        [(tiles, bf16)] * 2,
        scratch=[
            pltpu.VMEM(tiles, f32),
            pltpu.VMEM((slots, width), bf16),
            pltpu.VMEM((slots, width), bf16),
            pltpu.VMEM((2 * tiles[0], lanes), f32),
        ],
        kinds=[vmem] * 5,
    )(arrived, other, gate_weight, up_weight, down_weight)
    got = swap_tp(given)
    answered = (kept.astype(f32) + got.astype(f32)).astype(bf16)
    returned = exchange(answered.reshape(wire)).reshape(slots, width)

    def blended(blend):
        return lax.dot_general(
            blend, returned, (((0,), (0,)), ((), ())), preferred_element_type=f32
        )

    return (blended(high) + blended(low)).astype(bf16)


def solution(mesh):
    placed = (
        P(("grp", "ep"), "tp"),
        P(("grp", "ep"), None),
        P(("grp", "ep"), None),
        P("tp"),
        P("tp"),
        P("ep", None, "tp"),
        P("ep", None, "tp"),
        P("ep", "tp", None),
    )
    return jax.shard_map(
        body, mesh=mesh, in_specs=placed, out_specs=P(("grp", "ep"), "tp"), check_vma=False
    )
```

```python
import functools

import jax
import jax.numpy as jnp
from jax import lax
from jax.experimental import pallas as pl
from jax.experimental.pallas import tpu as pltpu
from jax.sharding import PartitionSpec as P

norm_eps = 1e-05
clamp_limit = 7.0
sigmoid_slope = 1.702
lanes = 128


def swap_tp(x):
    return lax.ppermute(x, "tp", [(0, 1), (1, 0)])


def exchange(x):
    return lax.all_to_all(x, "ep", split_axis=0, concat_axis=0, tiled=True)


def in_kernel(name, kernel, outs, scratch, kinds):
    vmem = pl.BlockSpec(memory_space=pltpu.VMEM)
    return pl.pallas_call(
        kernel,
        out_shape=tuple(jax.ShapeDtypeStruct(shape, dtype) for shape, dtype in outs),
        in_specs=[pl.BlockSpec(memory_space=kind) for kind in kinds],
        out_specs=tuple(vmem for _ in outs),
        scratch_shapes=list(scratch),
        compiler_params=pltpu.CompilerParams(vmem_limit_bytes=16 << 20),
        name=name,
    )


def in_hbm(x):
    return pltpu.with_memory_space_constraint(x, pltpu.HBM)


def start_all(pairs, sems):
    copies = [pltpu.make_async_copy(*pair, sems.at[i]) for i, pair in enumerate(pairs)]
    for copy in copies:
        copy.start()
    return copies


def pack_kernel(capacity, routes_hbm, logits_hbm, tokens_hbm, gain_hbm, shift_hbm, gate_hbm, packed_ref, high_ref, low_ref, affine_ref, gate_ref, routes_ref, logits_ref, tokens_ref, wide, sems):
    top_count, rows = routes_ref.shape
    slots = high_ref.shape[0]
    experts = slots // capacity
    blocks = tokens_ref.shape[1] // lanes
    copies = start_all(
        (
            (routes_hbm, routes_ref),
            (logits_hbm, logits_ref),
            (tokens_hbm, tokens_ref),
            (gain_hbm, affine_ref.at[0:blocks]),
            (shift_hbm, affine_ref.at[blocks : 2 * blocks]),
            (gate_hbm, gate_ref),
        ),
        sems,
    )
    copies[0].wait()
    expert_id = lax.broadcasted_iota(jnp.int32, (experts, rows), 0)
    matches = [routes_ref[k : k + 1, :] == expert_id for k in range(top_count)]
    chosen = functools.reduce(jnp.logical_or, matches)
    earlier = lax.broadcasted_iota(jnp.int32, (rows, rows), 0) < lax.broadcasted_iota(
        jnp.int32, (rows, rows), 1
    )
    rank = jnp.dot(
        jnp.where(chosen, 1.0, 0.0).astype(jnp.bfloat16),
        jnp.where(earlier, 1.0, 0.0).astype(jnp.bfloat16),
        preferred_element_type=jnp.float32,
    )
    slot_of = jnp.where(
        chosen, rank + (expert_id * capacity).astype(jnp.float32), -1.0
    ).astype(jnp.bfloat16)
    slot_id = lax.broadcasted_iota(jnp.int32, (slots, experts), 0)
    first = lax.broadcasted_iota(jnp.int32, (slots, experts), 1) * capacity
    spread = jnp.where((slot_id >= first) & (slot_id < first + capacity), 1.0, 0.0).astype(
        jnp.bfloat16
    )

    def to_slots(x):
        return jnp.dot(spread, x, preferred_element_type=jnp.float32)

    taken = to_slots(slot_of) == lax.broadcasted_iota(jnp.int32, (slots, rows), 0).astype(jnp.float32)
    pick = jnp.where(taken, 1.0, 0.0).astype(jnp.bfloat16)
    copies[2].wait()
    packed = jnp.dot(pick, tokens_ref[...], preferred_element_type=jnp.float32)
    for j in range(blocks):
        wide[pl.ds(j, slots, stride=blocks), :] = packed[:, j * lanes : (j + 1) * lanes]
    packed_ref[...] = wide[...].astype(jnp.bfloat16)
    copies[1].wait()
    exp_logits = jnp.exp(logits_ref[...])
    weights = exp_logits / jnp.sum(exp_logits, axis=0, keepdims=True)
    weight_of = jnp.zeros((experts, rows), jnp.float32)
    for k, match in enumerate(matches):
        weight_of = jnp.where(match, weights[k : k + 1, :], weight_of)
    high = weight_of.astype(jnp.bfloat16)
    low = (weight_of - high.astype(jnp.float32)).astype(jnp.bfloat16)
    high_ref[...] = jnp.where(taken, to_slots(high), 0.0).astype(jnp.bfloat16)
    low_ref[...] = jnp.where(taken, to_slots(low), 0.0).astype(jnp.bfloat16)
    for copy in copies[3:]:
        copy.wait()


def unpack(tiles_ref, rows_ref, sums_ref, wide):
    slots, width = rows_ref.shape
    blocks = width // lanes
    wide[...] = tiles_ref[...].astype(jnp.float32)
    total = jnp.zeros((slots, lanes), jnp.float32)
    squares = jnp.zeros((slots, lanes), jnp.float32)
    for j in range(blocks):
        part = wide[pl.ds(j, slots, stride=blocks), :]
        rows_ref[:, j * lanes : (j + 1) * lanes] = part.astype(jnp.bfloat16)
        total = total + part
        squares = squares + part * part
    sums_ref[:slots, :] = total
    sums_ref[slots:, :] = squares


def own_kernel(own_ref, up_hbm, rows_ref, sums_ref, up_ref, wide, sems):
    copies = start_all(((up_hbm, up_ref),), sems)
    unpack(own_ref, rows_ref, sums_ref, wide)
    copies[0].wait()


def give(part, wide, out_ref):
    slots = part.shape[0]
    blocks = part.shape[1] // lanes
    for j in range(blocks):
        wide[pl.ds(j, slots, stride=blocks), :] = part[:, j * lanes : (j + 1) * lanes]
    out_ref[...] = wide[...].astype(jnp.bfloat16)


def expert_kernel(rows_own, own_sums, other_ref, own_affine, other_affine, gate_ref, up_ref, down_hbm, hidden_ref, given_ref, wide, rows_other, other_sums, down_ref, sems):
    slots, width = rows_own.shape
    blocks = width // lanes
    half = lax.axis_index("tp")
    here = pl.multiple_of(half * width, width)
    there = pl.multiple_of((1 - half) * width, width)
    copies = start_all(((down_hbm.at[0, :, pl.ds(there, width)], down_ref),), sems)
    unpack(other_ref, rows_other, other_sums, wide)
    sums = jnp.sum(own_sums[...] + other_sums[...], axis=1, keepdims=True)
    average = sums[:slots, :] / (2 * width)
    variance = sums[slots:, :] / (2 * width) - average * average
    inverse = lax.rsqrt(variance + norm_eps)

    def normalised(rows_ref, affine_ref):
        return jnp.concatenate(
            [
                (
                    (rows_ref[:, j * lanes : (j + 1) * lanes].astype(jnp.float32) - average)
                    * inverse
                    * affine_ref[j : j + 1, :]
                    + affine_ref[blocks + j : blocks + j + 1, :]
                ).astype(jnp.bfloat16)
                for j in range(blocks)
            ],
            axis=1,
        )

    own = normalised(rows_own, own_affine)
    other = normalised(rows_other, other_affine)

    def project(weight_ref):
        return jnp.dot(
            own, weight_ref[0, pl.ds(here, width), :], preferred_element_type=jnp.float32
        ) + jnp.dot(
            other, weight_ref[0, pl.ds(there, width), :], preferred_element_type=jnp.float32
        )

    gate_cut = jnp.minimum(project(gate_ref), clamp_limit)
    up_cut = jnp.clip(project(up_ref), -clamp_limit, clamp_limit)
    hidden = ((up_cut + 1.0) * gate_cut * jax.nn.sigmoid(sigmoid_slope * gate_cut)).astype(
        jnp.bfloat16
    )
    hidden_ref[...] = hidden
    copies[0].wait()
    give(jnp.dot(hidden, down_ref[...], preferred_element_type=jnp.float32), wide, given_ref)


def kept_kernel(hidden_ref, down_hbm, kept_ref, wide, down_ref, sems):
    width = down_ref.shape[1]
    here = pl.multiple_of(lax.axis_index("tp") * width, width)
    copies = start_all(((down_hbm.at[0, :, pl.ds(here, width)], down_ref),), sems)
    copies[0].wait()
    give(jnp.dot(hidden_ref[...], down_ref[...], preferred_element_type=jnp.float32), wide, kept_ref)


def body(tokens, routes, gate_logits, norm_gain, norm_shift, gate_weight, up_weight, down_weight):
    experts = lax.axis_size("ep")
    rows, top_count = routes.shape
    width = tokens.shape[1]
    capacity = rows * top_count // experts + 2
    blocks = width // lanes
    slots = experts * capacity
    wire = (experts, capacity * blocks, lanes)
    tiles = (slots * blocks, lanes)
    bf16, f32 = jnp.bfloat16, jnp.float32
    vmem, hbm = pltpu.VMEM, pltpu.HBM

    packed, high, low, affine, gate_weight = in_kernel(
        "pack",
        functools.partial(pack_kernel, capacity),
        [
            (tiles, bf16),
            ((slots, rows), bf16),
            ((slots, rows), bf16),
            ((2 * blocks, lanes), f32),
            (gate_weight.shape, bf16),
        ],
        scratch=[
            pltpu.VMEM((top_count, rows), jnp.int32),
            pltpu.VMEM((top_count, rows), f32),
            pltpu.VMEM(tokens.shape, bf16),
            pltpu.VMEM(tiles, f32),
            pltpu.SemaphoreType.DMA((6,)),
        ],
        kinds=[hbm] * 6,
    )(
        in_hbm(routes.T),
        in_hbm(gate_logits.T),
        in_hbm(tokens),
        in_hbm(norm_gain.reshape(blocks, lanes)),
        in_hbm(norm_shift.reshape(blocks, lanes)),
        in_hbm(gate_weight),
    )
    arrived = exchange(packed.reshape(wire)).reshape(tiles)
    arrived, affine = lax.optimization_barrier((arrived, affine))
    other = swap_tp(arrived)
    other_affine = swap_tp(affine)
    rows_own, own_sums, up_weight = in_kernel(
        "own",
        own_kernel,
        [((slots, width), bf16), ((2 * slots, lanes), f32), (up_weight.shape, bf16)],
        scratch=[pltpu.VMEM(tiles, f32), pltpu.SemaphoreType.DMA((1,))],
        kinds=[vmem, hbm],
    )(arrived, in_hbm(up_weight))
    down_half = pltpu.VMEM((down_weight.shape[1], width), bf16)
    hidden, given = in_kernel(
        "expert",
        expert_kernel,
        [((slots, gate_weight.shape[2]), bf16), (tiles, bf16)],
        scratch=[
            pltpu.VMEM(tiles, f32),
            pltpu.VMEM((slots, width), bf16),
            pltpu.VMEM((2 * slots, lanes), f32),
            down_half,
            pltpu.SemaphoreType.DMA((1,)),
        ],
        kinds=[vmem] * 7 + [hbm],
    )(rows_own, own_sums, other, affine, other_affine, gate_weight, up_weight, in_hbm(down_weight))
    (kept,) = in_kernel(
        "kept",
        kept_kernel,
        [(tiles, bf16)],
        scratch=[pltpu.VMEM(tiles, f32), down_half, pltpu.SemaphoreType.DMA((1,))],
        kinds=[vmem, hbm],
    )(hidden, in_hbm(down_weight))
    got = swap_tp(given)
    answered = (kept.astype(f32) + got.astype(f32)).astype(bf16)
    returned = exchange(answered.reshape(wire)).reshape(slots, width)

    def blended(blend):
        return lax.dot_general(
            blend, returned, (((0,), (0,)), ((), ())), preferred_element_type=f32
        )

    return (blended(high) + blended(low)).astype(bf16)


def solution(mesh):
    placed = (
        P(("grp", "ep"), "tp"),
        P(("grp", "ep"), None),
        P(("grp", "ep"), None),
        P("tp"),
        P("tp"),
        P("ep", None, "tp"),
        P("ep", None, "tp"),
        P("ep", "tp", None),
    )
    return jax.shard_map(
        body, mesh=mesh, in_specs=placed, out_specs=P(("grp", "ep"), "tp"), check_vma=False
    )
```

```python
import functools

import jax
import jax.numpy as jnp
from jax import lax
from jax.experimental import pallas as pl
from jax.experimental.pallas import tpu as pltpu
from jax.sharding import PartitionSpec as P

norm_eps = 1e-05
clamp_limit = 7.0
sigmoid_slope = 1.702
lanes = 128


def swap_tp(x):
    return lax.ppermute(x, "tp", [(0, 1), (1, 0)])


def ring_order():
    count = lax.axis_size("ep")
    return [(3 * count // 4 + k) % count for k in range(count)]


def exchange(x):
    return lax.all_to_all(
        x, "ep", split_axis=0, concat_axis=0, axis_index_groups=[ring_order()], tiled=True
    )


def in_kernel(name, kernel, outs, scratch, kinds):
    vmem = pl.BlockSpec(memory_space=pltpu.VMEM)
    return pl.pallas_call(
        kernel,
        out_shape=tuple(jax.ShapeDtypeStruct(shape, dtype) for shape, dtype in outs),
        in_specs=[pl.BlockSpec(memory_space=kind) for kind in kinds],
        out_specs=tuple(vmem for _ in outs),
        scratch_shapes=list(scratch),
        compiler_params=pltpu.CompilerParams(vmem_limit_bytes=16 << 20),
        name=name,
    )


def in_hbm(x):
    return pltpu.with_memory_space_constraint(x, pltpu.HBM)


def start_all(pairs, sems):
    copies = [pltpu.make_async_copy(*pair, sems.at[i]) for i, pair in enumerate(pairs)]
    for copy in copies:
        copy.start()
    return copies


def pack_kernel(capacity, first_expert, routes_hbm, logits_hbm, tokens_hbm, gain_hbm, shift_hbm, gate_hbm, packed_ref, high_ref, low_ref, affine_ref, gate_ref, routes_ref, logits_ref, tokens_ref, wide, sems):
    top_count, rows = routes_ref.shape
    slots = high_ref.shape[0]
    experts = slots // capacity
    blocks = tokens_ref.shape[1] // lanes
    copies = start_all(
        (
            (routes_hbm, routes_ref),
            (logits_hbm, logits_ref),
            (tokens_hbm, tokens_ref),
            (gain_hbm, affine_ref.at[0:blocks]),
            (shift_hbm, affine_ref.at[blocks : 2 * blocks]),
            (gate_hbm, gate_ref),
        ),
        sems,
    )
    copies[0].wait()
    expert_id = (lax.broadcasted_iota(jnp.int32, (experts, rows), 0) + first_expert) % experts
    place = lax.broadcasted_iota(jnp.int32, (experts, rows), 0) * capacity
    matches = [routes_ref[k : k + 1, :] == expert_id for k in range(top_count)]
    chosen = functools.reduce(jnp.logical_or, matches)
    earlier = lax.broadcasted_iota(jnp.int32, (rows, rows), 0) < lax.broadcasted_iota(
        jnp.int32, (rows, rows), 1
    )
    rank = jnp.dot(
        jnp.where(chosen, 1.0, 0.0).astype(jnp.bfloat16),
        jnp.where(earlier, 1.0, 0.0).astype(jnp.bfloat16),
        preferred_element_type=jnp.float32,
    )
    slot_of = jnp.where(
        chosen, rank + place.astype(jnp.float32), -1.0
    ).astype(jnp.bfloat16)
    slot_id = lax.broadcasted_iota(jnp.int32, (slots, experts), 0)
    first = lax.broadcasted_iota(jnp.int32, (slots, experts), 1) * capacity
    spread = jnp.where((slot_id >= first) & (slot_id < first + capacity), 1.0, 0.0).astype(
        jnp.bfloat16
    )

    def to_slots(x):
        return jnp.dot(spread, x, preferred_element_type=jnp.float32)

    taken = to_slots(slot_of) == lax.broadcasted_iota(jnp.int32, (slots, rows), 0).astype(jnp.float32)
    pick = jnp.where(taken, 1.0, 0.0).astype(jnp.bfloat16)
    copies[2].wait()
    packed = jnp.dot(pick, tokens_ref[...], preferred_element_type=jnp.float32)
    for j in range(blocks):
        wide[pl.ds(j, slots, stride=blocks), :] = packed[:, j * lanes : (j + 1) * lanes]
    packed_ref[...] = wide[...].astype(jnp.bfloat16)
    copies[1].wait()
    exp_logits = jnp.exp(logits_ref[...])
    weights = exp_logits / jnp.sum(exp_logits, axis=0, keepdims=True)
    weight_of = jnp.zeros((experts, rows), jnp.float32)
    for k, match in enumerate(matches):
        weight_of = jnp.where(match, weights[k : k + 1, :], weight_of)
    high = weight_of.astype(jnp.bfloat16)
    low = (weight_of - high.astype(jnp.float32)).astype(jnp.bfloat16)
    high_ref[...] = jnp.where(taken, to_slots(high), 0.0).astype(jnp.bfloat16)
    low_ref[...] = jnp.where(taken, to_slots(low), 0.0).astype(jnp.bfloat16)
    for copy in copies[3:]:
        copy.wait()


def unpack(tiles_ref, rows_ref, sums_ref, wide):
    slots, width = rows_ref.shape
    blocks = width // lanes
    wide[...] = tiles_ref[...].astype(jnp.float32)
    total = jnp.zeros((slots, lanes), jnp.float32)
    squares = jnp.zeros((slots, lanes), jnp.float32)
    for j in range(blocks):
        part = wide[pl.ds(j, slots, stride=blocks), :]
        rows_ref[:, j * lanes : (j + 1) * lanes] = part.astype(jnp.bfloat16)
        total = total + part
        squares = squares + part * part
    sums_ref[:slots, :] = total
    sums_ref[slots:, :] = squares


def own_kernel(own_ref, up_hbm, rows_ref, sums_ref, up_ref, wide, sems):
    copies = start_all(((up_hbm, up_ref),), sems)
    unpack(own_ref, rows_ref, sums_ref, wide)
    copies[0].wait()


def give(part, wide, out_ref):
    slots = part.shape[0]
    blocks = part.shape[1] // lanes
    for j in range(blocks):
        wide[pl.ds(j, slots, stride=blocks), :] = part[:, j * lanes : (j + 1) * lanes]
    out_ref[...] = wide[...].astype(jnp.bfloat16)


def expert_kernel(rows_own, own_sums, other_ref, own_affine, other_affine, gate_ref, up_ref, down_hbm, hidden_ref, given_ref, wide, rows_other, other_sums, down_ref, sems):
    slots, width = rows_own.shape
    blocks = width // lanes
    half = lax.axis_index("tp")
    here = pl.multiple_of(half * width, width)
    there = pl.multiple_of((1 - half) * width, width)
    copies = start_all(((down_hbm.at[0, :, pl.ds(there, width)], down_ref),), sems)
    unpack(other_ref, rows_other, other_sums, wide)
    sums = jnp.sum(own_sums[...] + other_sums[...], axis=1, keepdims=True)
    average = sums[:slots, :] / (2 * width)
    variance = sums[slots:, :] / (2 * width) - average * average
    inverse = lax.rsqrt(variance + norm_eps)

    def normalised(rows_ref, affine_ref):
        return jnp.concatenate(
            [
                (
                    (rows_ref[:, j * lanes : (j + 1) * lanes].astype(jnp.float32) - average)
                    * inverse
                    * affine_ref[j : j + 1, :]
                    + affine_ref[blocks + j : blocks + j + 1, :]
                ).astype(jnp.bfloat16)
                for j in range(blocks)
            ],
            axis=1,
        )

    own = normalised(rows_own, own_affine)
    other = normalised(rows_other, other_affine)

    def project(weight_ref):
        return jnp.dot(
            own, weight_ref[0, pl.ds(here, width), :], preferred_element_type=jnp.float32
        ) + jnp.dot(
            other, weight_ref[0, pl.ds(there, width), :], preferred_element_type=jnp.float32
        )

    gate_cut = jnp.minimum(project(gate_ref), clamp_limit)
    up_cut = jnp.clip(project(up_ref), -clamp_limit, clamp_limit)
    hidden = ((up_cut + 1.0) * gate_cut * jax.nn.sigmoid(sigmoid_slope * gate_cut)).astype(
        jnp.bfloat16
    )
    hidden_ref[...] = hidden
    copies[0].wait()
    give(jnp.dot(hidden, down_ref[...], preferred_element_type=jnp.float32), wide, given_ref)


def kept_kernel(hidden_ref, down_hbm, kept_ref, wide, down_ref, sems):
    width = down_ref.shape[1]
    here = pl.multiple_of(lax.axis_index("tp") * width, width)
    copies = start_all(((down_hbm.at[0, :, pl.ds(here, width)], down_ref),), sems)
    copies[0].wait()
    give(jnp.dot(hidden_ref[...], down_ref[...], preferred_element_type=jnp.float32), wide, kept_ref)


def body(tokens, routes, gate_logits, norm_gain, norm_shift, gate_weight, up_weight, down_weight):
    experts = lax.axis_size("ep")
    rows, top_count = routes.shape
    width = tokens.shape[1]
    capacity = rows * top_count // experts + 2
    blocks = width // lanes
    slots = experts * capacity
    wire = (experts, capacity * blocks, lanes)
    tiles = (slots * blocks, lanes)
    bf16, f32 = jnp.bfloat16, jnp.float32
    vmem, hbm = pltpu.VMEM, pltpu.HBM

    packed, high, low, affine, gate_weight = in_kernel(
        "pack",
        functools.partial(pack_kernel, capacity, ring_order()[0]),
        [
            (tiles, bf16),
            ((slots, rows), bf16),
            ((slots, rows), bf16),
            ((2 * blocks, lanes), f32),
            (gate_weight.shape, bf16),
        ],
        scratch=[
            pltpu.VMEM((top_count, rows), jnp.int32),
            pltpu.VMEM((top_count, rows), f32),
            pltpu.VMEM(tokens.shape, bf16),
            pltpu.VMEM(tiles, f32),
            pltpu.SemaphoreType.DMA((6,)),
        ],
        kinds=[hbm] * 6,
    )(
        in_hbm(routes.T),
        in_hbm(gate_logits.T),
        in_hbm(tokens),
        in_hbm(norm_gain.reshape(blocks, lanes)),
        in_hbm(norm_shift.reshape(blocks, lanes)),
        in_hbm(gate_weight),
    )
    arrived = exchange(packed.reshape(wire)).reshape(tiles)
    arrived, affine = lax.optimization_barrier((arrived, affine))
    other = swap_tp(arrived)
    other_affine = swap_tp(affine)
    rows_own, own_sums, up_weight = in_kernel(
        "own",
        own_kernel,
        [((slots, width), bf16), ((2 * slots, lanes), f32), (up_weight.shape, bf16)],
        scratch=[pltpu.VMEM(tiles, f32), pltpu.SemaphoreType.DMA((1,))],
        kinds=[vmem, hbm],
    )(arrived, in_hbm(up_weight))
    down_half = pltpu.VMEM((down_weight.shape[1], width), bf16)
    hidden, given = in_kernel(
        "expert",
        expert_kernel,
        [((slots, gate_weight.shape[2]), bf16), (tiles, bf16)],
        scratch=[
            pltpu.VMEM(tiles, f32),
            pltpu.VMEM((slots, width), bf16),
            pltpu.VMEM((2 * slots, lanes), f32),
            down_half,
            pltpu.SemaphoreType.DMA((1,)),
        ],
        kinds=[vmem] * 7 + [hbm],
    )(rows_own, own_sums, other, affine, other_affine, gate_weight, up_weight, in_hbm(down_weight))
    (kept,) = in_kernel(
        "kept",
        kept_kernel,
        [(tiles, bf16)],
        scratch=[pltpu.VMEM(tiles, f32), down_half, pltpu.SemaphoreType.DMA((1,))],
        kinds=[vmem, hbm],
    )(hidden, in_hbm(down_weight))
    got = swap_tp(given)
    answered = (kept.astype(f32) + got.astype(f32)).astype(bf16)
    returned = exchange(answered.reshape(wire)).reshape(slots, width)

    def blended(blend):
        return lax.dot_general(
            blend, returned, (((0,), (0,)), ((), ())), preferred_element_type=f32
        )

    return (blended(high) + blended(low)).astype(bf16)


def solution(mesh):
    placed = (
        P(("grp", "ep"), "tp"),
        P(("grp", "ep"), None),
        P(("grp", "ep"), None),
        P("tp"),
        P("tp"),
        P("ep", None, "tp"),
        P("ep", None, "tp"),
        P("ep", "tp", None),
    )
    return jax.shard_map(
        body, mesh=mesh, in_specs=placed, out_specs=P(("grp", "ep"), "tp"), check_vma=False
    )
```

```python
import functools

import jax
import jax.numpy as jnp
from jax import lax
from jax.experimental import pallas as pl
from jax.experimental.pallas import tpu as pltpu
from jax.sharding import PartitionSpec as P

norm_eps = 1e-05
clamp_limit = 7.0
sigmoid_slope = 1.702
lanes = 128


def swap_tp(x):
    return lax.ppermute(x, "tp", [(0, 1), (1, 0)])


def ring_order():
    count = lax.axis_size("ep")
    return [(3 * count // 4 + k) % count for k in range(count)]


def exchange(x):
    return lax.all_to_all(
        x, "ep", split_axis=0, concat_axis=0, axis_index_groups=[ring_order()], tiled=True
    )


def in_kernel(name, kernel, outs, scratch, kinds):
    vmem = pl.BlockSpec(memory_space=pltpu.VMEM)
    return pl.pallas_call(
        kernel,
        out_shape=tuple(jax.ShapeDtypeStruct(shape, dtype) for shape, dtype in outs),
        in_specs=[pl.BlockSpec(memory_space=kind) for kind in kinds],
        out_specs=tuple(vmem for _ in outs),
        scratch_shapes=list(scratch),
        compiler_params=pltpu.CompilerParams(vmem_limit_bytes=16 << 20),
        name=name,
    )


def in_hbm(x):
    return pltpu.with_memory_space_constraint(x, pltpu.HBM)


def start_all(pairs, sems):
    copies = [pltpu.make_async_copy(*pair, sems.at[i]) for i, pair in enumerate(pairs)]
    for copy in copies:
        copy.start()
    return copies


def expert_ids(experts, rows, first_expert):
    return (lax.broadcasted_iota(jnp.int32, (experts, rows), 0) + first_expert) % experts


def spread_of(slots, experts, capacity):
    slot_id = lax.broadcasted_iota(jnp.int32, (slots, experts), 0)
    first = lax.broadcasted_iota(jnp.int32, (slots, experts), 1) * capacity
    return jnp.where((slot_id >= first) & (slot_id < first + capacity), 1.0, 0.0).astype(
        jnp.bfloat16
    )


def pack_kernel(capacity, first_expert, routes_hbm, logits_hbm, tokens_hbm, gain_hbm, shift_hbm, gate_hbm, packed_ref, pick_ref, affine_ref, gate_ref, routes_ref, logits_ref, tokens_ref, wide, sems):
    top_count, rows = routes_ref.shape
    slots = pick_ref.shape[0]
    experts = slots // capacity
    blocks = tokens_ref.shape[1] // lanes
    copies = start_all(
        (
            (routes_hbm, routes_ref),
            (logits_hbm, logits_ref),
            (tokens_hbm, tokens_ref),
            (gain_hbm, affine_ref.at[0:blocks]),
            (shift_hbm, affine_ref.at[blocks : 2 * blocks]),
            (gate_hbm, gate_ref),
        ),
        sems,
    )
    copies[0].wait()
    expert_id = expert_ids(experts, rows, first_expert)
    place = lax.broadcasted_iota(jnp.int32, (experts, rows), 0) * capacity
    matches = [routes_ref[k : k + 1, :] == expert_id for k in range(top_count)]
    chosen = functools.reduce(jnp.logical_or, matches)
    earlier = lax.broadcasted_iota(jnp.int32, (rows, rows), 0) < lax.broadcasted_iota(
        jnp.int32, (rows, rows), 1
    )
    rank = jnp.dot(
        jnp.where(chosen, 1.0, 0.0).astype(jnp.bfloat16),
        jnp.where(earlier, 1.0, 0.0).astype(jnp.bfloat16),
        preferred_element_type=jnp.float32,
    )
    slot_of = jnp.where(
        chosen, rank + place.astype(jnp.float32), -1.0
    ).astype(jnp.bfloat16)
    spread = spread_of(slots, experts, capacity)
    at_slots = jnp.dot(spread, slot_of, preferred_element_type=jnp.float32)
    taken = at_slots == lax.broadcasted_iota(jnp.int32, (slots, rows), 0).astype(jnp.float32)
    pick = jnp.where(taken, 1.0, 0.0).astype(jnp.bfloat16)
    pick_ref[...] = pick
    copies[2].wait()
    packed = jnp.dot(pick, tokens_ref[...], preferred_element_type=jnp.float32)
    for j in range(blocks):
        wide[pl.ds(j, slots, stride=blocks), :] = packed[:, j * lanes : (j + 1) * lanes]
    packed_ref[...] = wide[...].astype(jnp.bfloat16)
    copies[1].wait()
    for copy in copies[3:]:
        copy.wait()


def unpack(tiles_ref, rows_ref, sums_ref, wide):
    slots, width = rows_ref.shape
    blocks = width // lanes
    wide[...] = tiles_ref[...].astype(jnp.float32)
    total = jnp.zeros((slots, lanes), jnp.float32)
    squares = jnp.zeros((slots, lanes), jnp.float32)
    for j in range(blocks):
        part = wide[pl.ds(j, slots, stride=blocks), :]
        rows_ref[:, j * lanes : (j + 1) * lanes] = part.astype(jnp.bfloat16)
        total = total + part
        squares = squares + part * part
    sums_ref[:slots, :] = total
    sums_ref[slots:, :] = squares


def own_kernel(own_ref, up_hbm, rows_ref, sums_ref, up_ref, wide, sems):
    copies = start_all(((up_hbm, up_ref),), sems)
    unpack(own_ref, rows_ref, sums_ref, wide)
    copies[0].wait()


def give(part, wide, out_ref):
    slots = part.shape[0]
    blocks = part.shape[1] // lanes
    for j in range(blocks):
        wide[pl.ds(j, slots, stride=blocks), :] = part[:, j * lanes : (j + 1) * lanes]
    out_ref[...] = wide[...].astype(jnp.bfloat16)


def expert_kernel(rows_own, own_sums, other_ref, own_affine, other_affine, gate_ref, up_ref, down_hbm, hidden_ref, given_ref, down_kept, wide, rows_other, other_sums, down_given, sems):
    slots, width = rows_own.shape
    blocks = width // lanes
    half = lax.axis_index("tp")
    here = pl.multiple_of(half * width, width)
    there = pl.multiple_of((1 - half) * width, width)
    copies = start_all(
        (
            (down_hbm.at[0, :, pl.ds(there, width)], down_given),
            (down_hbm.at[0, :, pl.ds(here, width)], down_kept),
        ),
        sems,
    )
    unpack(other_ref, rows_other, other_sums, wide)
    sums = jnp.sum(own_sums[...] + other_sums[...], axis=1, keepdims=True)
    average = sums[:slots, :] / (2 * width)
    variance = sums[slots:, :] / (2 * width) - average * average
    inverse = jnp.broadcast_to(lax.rsqrt(variance + norm_eps), (slots, lanes))
    average = jnp.broadcast_to(average, (slots, lanes))

    def normalised(rows_ref, affine_ref):
        return jnp.concatenate(
            [
                (
                    (rows_ref[:, j * lanes : (j + 1) * lanes].astype(jnp.float32) - average)
                    * inverse
                    * affine_ref[j : j + 1, :]
                    + affine_ref[blocks + j : blocks + j + 1, :]
                ).astype(jnp.bfloat16)
                for j in range(blocks)
            ],
            axis=1,
        )

    own = normalised(rows_own, own_affine)
    other = normalised(rows_other, other_affine)

    def project(weight_ref):
        return jnp.dot(
            own, weight_ref[0, pl.ds(here, width), :], preferred_element_type=jnp.float32
        ) + jnp.dot(
            other, weight_ref[0, pl.ds(there, width), :], preferred_element_type=jnp.float32
        )

    gate_cut = jnp.minimum(project(gate_ref), clamp_limit)
    up_cut = jnp.clip(project(up_ref), -clamp_limit, clamp_limit)
    hidden = ((up_cut + 1.0) * gate_cut * jax.nn.sigmoid(sigmoid_slope * gate_cut)).astype(
        jnp.bfloat16
    )
    hidden_ref[...] = hidden
    copies[0].wait()
    give(jnp.dot(hidden, down_given[...], preferred_element_type=jnp.float32), wide, given_ref)
    copies[1].wait()


def kept_kernel(capacity, first_expert, hidden_ref, down_ref, routes_ref, logits_ref, pick_ref, kept_ref, high_ref, low_ref, wide):
    give(jnp.dot(hidden_ref[...], down_ref[...], preferred_element_type=jnp.float32), wide, kept_ref)
    top_count, rows = routes_ref.shape
    slots = pick_ref.shape[0]
    experts = slots // capacity
    exp_logits = jnp.exp(logits_ref[...])
    weights = exp_logits / jnp.sum(exp_logits, axis=0, keepdims=True)
    expert_id = expert_ids(experts, rows, first_expert)
    weight_of = jnp.zeros((experts, rows), jnp.float32)
    for k in range(top_count):
        weight_of = jnp.where(routes_ref[k : k + 1, :] == expert_id, weights[k : k + 1, :], weight_of)
    high = weight_of.astype(jnp.bfloat16)
    low = (weight_of - high.astype(jnp.float32)).astype(jnp.bfloat16)
    spread = spread_of(slots, experts, capacity)
    taken = pick_ref[...].astype(jnp.float32) > 0.0
    for part, part_ref in ((high, high_ref), (low, low_ref)):
        at_slots = jnp.dot(spread, part, preferred_element_type=jnp.float32)
        part_ref[...] = jnp.where(taken, at_slots, 0.0).astype(jnp.bfloat16)


def body(tokens, routes, gate_logits, norm_gain, norm_shift, gate_weight, up_weight, down_weight):
    experts = lax.axis_size("ep")
    rows, top_count = routes.shape
    width = tokens.shape[1]
    capacity = rows * top_count // experts + 2
    blocks = width // lanes
    slots = experts * capacity
    wire = (experts, capacity * blocks, lanes)
    tiles = (slots * blocks, lanes)
    bf16, f32 = jnp.bfloat16, jnp.float32
    vmem, hbm = pltpu.VMEM, pltpu.HBM

    packed, pick, affine, gate_weight, routes, gate_logits = in_kernel(
        "pack",
        functools.partial(pack_kernel, capacity, ring_order()[0]),
        [
            (tiles, bf16),
            ((slots, rows), bf16),
            ((2 * blocks, lanes), f32),
            (gate_weight.shape, bf16),
            ((top_count, rows), jnp.int32),
            ((top_count, rows), f32),
        ],
        scratch=[
            pltpu.VMEM(tokens.shape, bf16),
            pltpu.VMEM(tiles, f32),
            pltpu.SemaphoreType.DMA((6,)),
        ],
        kinds=[hbm] * 6,
    )(
        in_hbm(routes.T),
        in_hbm(gate_logits.T),
        in_hbm(tokens),
        in_hbm(norm_gain.reshape(blocks, lanes)),
        in_hbm(norm_shift.reshape(blocks, lanes)),
        in_hbm(gate_weight),
    )
    arrived = exchange(packed.reshape(wire)).reshape(tiles)
    arrived, affine = lax.optimization_barrier((arrived, affine))
    other = swap_tp(arrived)
    other_affine = swap_tp(affine)
    rows_own, own_sums, up_weight = in_kernel(
        "own",
        own_kernel,
        [((slots, width), bf16), ((2 * slots, lanes), f32), (up_weight.shape, bf16)],
        scratch=[pltpu.VMEM(tiles, f32), pltpu.SemaphoreType.DMA((1,))],
        kinds=[vmem, hbm],
    )(arrived, in_hbm(up_weight))
    down_half = (down_weight.shape[1], width)
    hidden, given, down_kept = in_kernel(
        "expert",
        expert_kernel,
        [((slots, gate_weight.shape[2]), bf16), (tiles, bf16), (down_half, bf16)],
        scratch=[
            pltpu.VMEM(tiles, f32),
            pltpu.VMEM((slots, width), bf16),
            pltpu.VMEM((2 * slots, lanes), f32),
            pltpu.VMEM(down_half, bf16),
            pltpu.SemaphoreType.DMA((2,)),
        ],
        kinds=[vmem] * 7 + [hbm],
    )(rows_own, own_sums, other, affine, other_affine, gate_weight, up_weight, in_hbm(down_weight))
    kept, high, low = in_kernel(
        "kept",
        functools.partial(kept_kernel, capacity, ring_order()[0]),
        [(tiles, bf16), ((slots, rows), bf16), ((slots, rows), bf16)],
        scratch=[pltpu.VMEM(tiles, f32)],
        kinds=[vmem] * 5,
    )(hidden, down_kept, routes, gate_logits, pick)
    got = swap_tp(given)
    answered = (kept.astype(f32) + got.astype(f32)).astype(bf16)
    returned = exchange(answered.reshape(wire)).reshape(slots, width)

    def blended(blend):
        return lax.dot_general(
            blend, returned, (((0,), (0,)), ((), ())), preferred_element_type=f32
        )

    return (blended(high) + blended(low)).astype(bf16)


def solution(mesh):
    placed = (
        P(("grp", "ep"), "tp"),
        P(("grp", "ep"), None),
        P(("grp", "ep"), None),
        P("tp"),
        P("tp"),
        P("ep", None, "tp"),
        P("ep", None, "tp"),
        P("ep", "tp", None),
    )
    return jax.shard_map(
        body, mesh=mesh, in_specs=placed, out_specs=P(("grp", "ep"), "tp"), check_vma=False
    )
```

```python
import functools

import jax
import jax.numpy as jnp
from jax import lax
from jax.experimental import pallas as pl
from jax.experimental.pallas import tpu as pltpu
from jax.sharding import PartitionSpec as P

norm_eps = 1e-05
clamp_limit = 7.0
sigmoid_slope = 1.702
lanes = 128


def swap_tp(x):
    return lax.ppermute(x, "tp", [(0, 1), (1, 0)])


def ring_order():
    count = lax.axis_size("ep")
    return [(3 * count // 4 + k) % count for k in range(count)]


def exchange(x):
    return lax.all_to_all(
        x, "ep", split_axis=0, concat_axis=0, axis_index_groups=[ring_order()], tiled=True
    )


def in_kernel(name, kernel, outs, scratch, kinds):
    vmem = pl.BlockSpec(memory_space=pltpu.VMEM)
    return pl.pallas_call(
        kernel,
        out_shape=tuple(jax.ShapeDtypeStruct(shape, dtype) for shape, dtype in outs),
        in_specs=[pl.BlockSpec(memory_space=kind) for kind in kinds],
        out_specs=tuple(vmem for _ in outs),
        scratch_shapes=list(scratch),
        compiler_params=pltpu.CompilerParams(vmem_limit_bytes=16 << 20),
        name=name,
    )


def in_hbm(x):
    return pltpu.with_memory_space_constraint(x, pltpu.HBM)


def start_all(pairs, sems):
    copies = [pltpu.make_async_copy(*pair, sems.at[i]) for i, pair in enumerate(pairs)]
    for copy in copies:
        copy.start()
    return copies


def expert_ids(experts, rows, first_expert):
    return (lax.broadcasted_iota(jnp.int32, (experts, rows), 0) + first_expert) % experts


def spread_of(slots, experts, capacity):
    slot_id = lax.broadcasted_iota(jnp.int32, (slots, experts), 0)
    first = lax.broadcasted_iota(jnp.int32, (slots, experts), 1) * capacity
    return jnp.where((slot_id >= first) & (slot_id < first + capacity), 1.0, 0.0).astype(
        jnp.bfloat16
    )


def pack_kernel(capacity, first_expert, routes_hbm, logits_hbm, tokens_hbm, gain_hbm, shift_hbm, gate_hbm, packed_ref, pick_ref, affine_ref, gate_ref, routes_ref, logits_ref, tokens_ref, wide, sems):
    top_count, rows = routes_ref.shape
    slots = pick_ref.shape[0]
    experts = slots // capacity
    width = tokens_ref.shape[1]
    blocks = width // lanes
    here = pl.multiple_of(lax.axis_index("tp") * width, width)
    copies = start_all(
        (
            (routes_hbm, routes_ref),
            (logits_hbm, logits_ref),
            (tokens_hbm, tokens_ref),
            (gain_hbm, affine_ref.at[0:blocks]),
            (shift_hbm, affine_ref.at[blocks : 2 * blocks]),
            (gate_hbm.at[0, pl.ds(here, width), :], gate_ref),
        ),
        sems,
    )
    copies[0].wait()
    expert_id = expert_ids(experts, rows, first_expert)
    place = lax.broadcasted_iota(jnp.int32, (experts, rows), 0) * capacity
    matches = [routes_ref[k : k + 1, :] == expert_id for k in range(top_count)]
    chosen = functools.reduce(jnp.logical_or, matches)
    earlier = lax.broadcasted_iota(jnp.int32, (rows, rows), 0) < lax.broadcasted_iota(
        jnp.int32, (rows, rows), 1
    )
    rank = jnp.dot(
        jnp.where(chosen, 1.0, 0.0).astype(jnp.bfloat16),
        jnp.where(earlier, 1.0, 0.0).astype(jnp.bfloat16),
        preferred_element_type=jnp.float32,
    )
    slot_of = jnp.where(
        chosen, rank + place.astype(jnp.float32), -1.0
    ).astype(jnp.bfloat16)
    spread = spread_of(slots, experts, capacity)
    at_slots = jnp.dot(spread, slot_of, preferred_element_type=jnp.float32)
    taken = at_slots == lax.broadcasted_iota(jnp.int32, (slots, rows), 0).astype(jnp.float32)
    pick = jnp.where(taken, 1.0, 0.0).astype(jnp.bfloat16)
    pick_ref[...] = pick
    copies[2].wait()
    packed = jnp.dot(pick, tokens_ref[...], preferred_element_type=jnp.float32)
    for j in range(blocks):
        wide[pl.ds(j, slots, stride=blocks), :] = packed[:, j * lanes : (j + 1) * lanes]
    packed_ref[...] = wide[...].astype(jnp.bfloat16)
    copies[1].wait()
    for copy in copies[3:]:
        copy.wait()


def unpack(tiles_ref, rows_ref, sums_ref, wide):
    slots, width = rows_ref.shape
    blocks = width // lanes
    wide[...] = tiles_ref[...].astype(jnp.float32)
    total = jnp.zeros((slots, lanes), jnp.float32)
    squares = jnp.zeros((slots, lanes), jnp.float32)
    for j in range(blocks):
        part = wide[pl.ds(j, slots, stride=blocks), :]
        rows_ref[:, j * lanes : (j + 1) * lanes] = part.astype(jnp.bfloat16)
        total = total + part
        squares = squares + part * part
    sums_ref[:slots, :] = total
    sums_ref[slots:, :] = squares


def own_kernel(own_ref, up_hbm, rows_ref, sums_ref, up_ref, wide, sems):
    copies = start_all(((up_hbm, up_ref),), sems)
    unpack(own_ref, rows_ref, sums_ref, wide)
    copies[0].wait()


def give(part, wide, out_ref):
    slots = part.shape[0]
    blocks = part.shape[1] // lanes
    for j in range(blocks):
        wide[pl.ds(j, slots, stride=blocks), :] = part[:, j * lanes : (j + 1) * lanes]
    out_ref[...] = wide[...].astype(jnp.bfloat16)


def expert_kernel(rows_own, own_sums, other_ref, own_affine, other_affine, gate_own, up_ref, gate_hbm, down_hbm, hidden_ref, given_ref, down_kept, wide, rows_other, other_sums, gate_other, down_given, sems):
    slots, width = rows_own.shape
    blocks = width // lanes
    half = lax.axis_index("tp")
    here = pl.multiple_of(half * width, width)
    there = pl.multiple_of((1 - half) * width, width)
    copies = start_all(
        (
            (gate_hbm.at[0, pl.ds(there, width), :], gate_other),
            (down_hbm.at[0, :, pl.ds(there, width)], down_given),
            (down_hbm.at[0, :, pl.ds(here, width)], down_kept),
        ),
        sems,
    )
    unpack(other_ref, rows_other, other_sums, wide)
    sums = jnp.sum(own_sums[...] + other_sums[...], axis=1, keepdims=True)
    average = sums[:slots, :] / (2 * width)
    variance = sums[slots:, :] / (2 * width) - average * average
    inverse = jnp.broadcast_to(lax.rsqrt(variance + norm_eps), (slots, lanes))
    average = jnp.broadcast_to(average, (slots, lanes))

    def normalised(rows_ref, affine_ref):
        return jnp.concatenate(
            [
                (
                    (rows_ref[:, j * lanes : (j + 1) * lanes].astype(jnp.float32) - average)
                    * inverse
                    * affine_ref[j : j + 1, :]
                    + affine_ref[blocks + j : blocks + j + 1, :]
                ).astype(jnp.bfloat16)
                for j in range(blocks)
            ],
            axis=1,
        )

    own = normalised(rows_own, own_affine)
    other = normalised(rows_other, other_affine)

    def project(own_weight, other_weight):
        return jnp.dot(own, own_weight, preferred_element_type=jnp.float32) + jnp.dot(
            other, other_weight, preferred_element_type=jnp.float32
        )

    up_pre = project(up_ref[0, pl.ds(here, width), :], up_ref[0, pl.ds(there, width), :])
    up_cut = jnp.clip(up_pre, -clamp_limit, clamp_limit)
    copies[0].wait()
    gate_cut = jnp.minimum(project(gate_own[...], gate_other[...]), clamp_limit)
    hidden = ((up_cut + 1.0) * gate_cut * jax.nn.sigmoid(sigmoid_slope * gate_cut)).astype(
        jnp.bfloat16
    )
    hidden_ref[...] = hidden
    copies[1].wait()
    give(jnp.dot(hidden, down_given[...], preferred_element_type=jnp.float32), wide, given_ref)
    copies[2].wait()


def kept_kernel(capacity, first_expert, hidden_ref, down_ref, routes_ref, logits_ref, pick_ref, kept_ref, high_ref, low_ref, wide):
    give(jnp.dot(hidden_ref[...], down_ref[...], preferred_element_type=jnp.float32), wide, kept_ref)
    top_count, rows = routes_ref.shape
    slots = pick_ref.shape[0]
    experts = slots // capacity
    exp_logits = jnp.exp(logits_ref[...])
    weights = exp_logits / jnp.sum(exp_logits, axis=0, keepdims=True)
    expert_id = expert_ids(experts, rows, first_expert)
    weight_of = jnp.zeros((experts, rows), jnp.float32)
    for k in range(top_count):
        weight_of = jnp.where(routes_ref[k : k + 1, :] == expert_id, weights[k : k + 1, :], weight_of)
    high = weight_of.astype(jnp.bfloat16)
    low = (weight_of - high.astype(jnp.float32)).astype(jnp.bfloat16)
    spread = spread_of(slots, experts, capacity)
    taken = pick_ref[...].astype(jnp.float32) > 0.0
    for part, part_ref in ((high, high_ref), (low, low_ref)):
        at_slots = jnp.dot(spread, part, preferred_element_type=jnp.float32)
        part_ref[...] = jnp.where(taken, at_slots, 0.0).astype(jnp.bfloat16)


def body(tokens, routes, gate_logits, norm_gain, norm_shift, gate_weight, up_weight, down_weight):
    experts = lax.axis_size("ep")
    rows, top_count = routes.shape
    width = tokens.shape[1]
    capacity = rows * top_count // experts + 2
    blocks = width // lanes
    slots = experts * capacity
    wire = (experts, capacity * blocks, lanes)
    tiles = (slots * blocks, lanes)
    bf16, f32 = jnp.bfloat16, jnp.float32
    vmem, hbm = pltpu.VMEM, pltpu.HBM

    gate_half = (width, gate_weight.shape[2])
    packed, pick, affine, gate_own, routes, gate_logits = in_kernel(
        "pack",
        functools.partial(pack_kernel, capacity, ring_order()[0]),
        [
            (tiles, bf16),
            ((slots, rows), bf16),
            ((2 * blocks, lanes), f32),
            (gate_half, bf16),
            ((top_count, rows), jnp.int32),
            ((top_count, rows), f32),
        ],
        scratch=[
            pltpu.VMEM(tokens.shape, bf16),
            pltpu.VMEM(tiles, f32),
            pltpu.SemaphoreType.DMA((6,)),
        ],
        kinds=[hbm] * 6,
    )(
        in_hbm(routes.T),
        in_hbm(gate_logits.T),
        in_hbm(tokens),
        in_hbm(norm_gain.reshape(blocks, lanes)),
        in_hbm(norm_shift.reshape(blocks, lanes)),
        in_hbm(gate_weight),
    )
    arrived = exchange(packed.reshape(wire)).reshape(tiles)
    arrived, affine = lax.optimization_barrier((arrived, affine))
    other = swap_tp(arrived)
    other_affine = swap_tp(affine)
    rows_own, own_sums, up_weight = in_kernel(
        "own",
        own_kernel,
        [((slots, width), bf16), ((2 * slots, lanes), f32), (up_weight.shape, bf16)],
        scratch=[pltpu.VMEM(tiles, f32), pltpu.SemaphoreType.DMA((1,))],
        kinds=[vmem, hbm],
    )(arrived, in_hbm(up_weight))
    down_half = (down_weight.shape[1], width)
    hidden, given, down_kept = in_kernel(
        "expert",
        expert_kernel,
        [((slots, gate_weight.shape[2]), bf16), (tiles, bf16), (down_half, bf16)],
        scratch=[
            pltpu.VMEM(tiles, f32),
            pltpu.VMEM((slots, width), bf16),
            pltpu.VMEM((2 * slots, lanes), f32),
            pltpu.VMEM(gate_half, bf16),
            pltpu.VMEM(down_half, bf16),
            pltpu.SemaphoreType.DMA((3,)),
        ],
        kinds=[vmem] * 7 + [hbm] * 2,
    )(
        rows_own,
        own_sums,
        other,
        affine,
        other_affine,
        gate_own,
        up_weight,
        in_hbm(gate_weight),
        in_hbm(down_weight),
    )
    kept, high, low = in_kernel(
        "kept",
        functools.partial(kept_kernel, capacity, ring_order()[0]),
        [(tiles, bf16), ((slots, rows), bf16), ((slots, rows), bf16)],
        scratch=[pltpu.VMEM(tiles, f32)],
        kinds=[vmem] * 5,
    )(hidden, down_kept, routes, gate_logits, pick)
    got = swap_tp(given)
    answered = (kept.astype(f32) + got.astype(f32)).astype(bf16)
    returned = exchange(answered.reshape(wire)).reshape(slots, width)

    def blended(blend):
        return lax.dot_general(
            blend, returned, (((0,), (0,)), ((), ())), preferred_element_type=f32
        )

    return (blended(high) + blended(low)).astype(bf16)


def solution(mesh):
    placed = (
        P(("grp", "ep"), "tp"),
        P(("grp", "ep"), None),
        P(("grp", "ep"), None),
        P("tp"),
        P("tp"),
        P("ep", None, "tp"),
        P("ep", None, "tp"),
        P("ep", "tp", None),
    )
    return jax.shard_map(
        body, mesh=mesh, in_specs=placed, out_specs=P(("grp", "ep"), "tp"), check_vma=False
    )
```

```python
import functools

import jax
import jax.numpy as jnp
from jax import lax
from jax.experimental import pallas as pl
from jax.experimental.pallas import tpu as pltpu
from jax.sharding import PartitionSpec as P

norm_eps = 1e-05
clamp_limit = 7.0
sigmoid_slope = 1.702
lanes = 128


def swap_tp(x):
    return lax.ppermute(x, "tp", [(0, 1), (1, 0)])


def ring_order():
    count = lax.axis_size("ep")
    return [(3 * count // 4 + k) % count for k in range(count)]


def exchange(x):
    return lax.all_to_all(
        x, "ep", split_axis=0, concat_axis=0, axis_index_groups=[ring_order()], tiled=True
    )


def in_kernel(name, kernel, outs, scratch, kinds):
    vmem = pl.BlockSpec(memory_space=pltpu.VMEM)
    return pl.pallas_call(
        kernel,
        out_shape=tuple(jax.ShapeDtypeStruct(shape, dtype) for shape, dtype in outs),
        in_specs=[pl.BlockSpec(memory_space=kind) for kind in kinds],
        out_specs=tuple(vmem for _ in outs),
        scratch_shapes=list(scratch),
        compiler_params=pltpu.CompilerParams(vmem_limit_bytes=16 << 20),
        name=name,
    )


def in_vmem(x):
    return pltpu.with_memory_space_constraint(x, pltpu.VMEM)


def in_hbm(x):
    return pltpu.with_memory_space_constraint(x, pltpu.HBM)


def start_all(pairs, sems):
    copies = [pltpu.make_async_copy(*pair, sems.at[i]) for i, pair in enumerate(pairs)]
    for copy in copies:
        copy.start()
    return copies


def expert_ids(experts, rows, first_expert):
    return (lax.broadcasted_iota(jnp.int32, (experts, rows), 0) + first_expert) % experts


def spread_of(slots, experts, capacity):
    slot_id = lax.broadcasted_iota(jnp.int32, (slots, experts), 0)
    first = lax.broadcasted_iota(jnp.int32, (slots, experts), 1) * capacity
    return jnp.where((slot_id >= first) & (slot_id < first + capacity), 1.0, 0.0).astype(
        jnp.bfloat16
    )


def pack_kernel(capacity, first_expert, routes_hbm, logits_hbm, tokens_hbm, gain_hbm, shift_hbm, packed_ref, pick_ref, affine_ref, routes_ref, logits_ref, tokens_ref, wide, sems):
    top_count, rows = routes_ref.shape
    slots = pick_ref.shape[0]
    experts = slots // capacity
    blocks = tokens_ref.shape[1] // lanes
    copies = start_all(
        (
            (routes_hbm, routes_ref),
            (logits_hbm, logits_ref),
            (tokens_hbm, tokens_ref),
            (gain_hbm, affine_ref.at[0:blocks]),
            (shift_hbm, affine_ref.at[blocks : 2 * blocks]),
        ),
        sems,
    )
    copies[0].wait()
    expert_id = expert_ids(experts, rows, first_expert)
    place = lax.broadcasted_iota(jnp.int32, (experts, rows), 0) * capacity
    matches = [routes_ref[k : k + 1, :] == expert_id for k in range(top_count)]
    chosen = functools.reduce(jnp.logical_or, matches)
    earlier = lax.broadcasted_iota(jnp.int32, (rows, rows), 0) < lax.broadcasted_iota(
        jnp.int32, (rows, rows), 1
    )
    rank = jnp.dot(
        jnp.where(chosen, 1.0, 0.0).astype(jnp.bfloat16),
        jnp.where(earlier, 1.0, 0.0).astype(jnp.bfloat16),
        preferred_element_type=jnp.float32,
    )
    slot_of = jnp.where(
        chosen, rank + place.astype(jnp.float32), -1.0
    ).astype(jnp.bfloat16)
    spread = spread_of(slots, experts, capacity)
    at_slots = jnp.dot(spread, slot_of, preferred_element_type=jnp.float32)
    taken = at_slots == lax.broadcasted_iota(jnp.int32, (slots, rows), 0).astype(jnp.float32)
    pick = jnp.where(taken, 1.0, 0.0).astype(jnp.bfloat16)
    pick_ref[...] = pick
    copies[2].wait()
    packed = jnp.dot(pick, tokens_ref[...], preferred_element_type=jnp.float32)
    for j in range(blocks):
        wide[pl.ds(j, slots, stride=blocks), :] = packed[:, j * lanes : (j + 1) * lanes]
    packed_ref[...] = wide[...].astype(jnp.bfloat16)
    copies[1].wait()
    for copy in copies[3:]:
        copy.wait()


def unpack(tiles_ref, rows_ref, sums_ref, wide):
    slots, width = rows_ref.shape
    blocks = width // lanes
    wide[...] = tiles_ref[...].astype(jnp.float32)
    total = jnp.zeros((slots, lanes), jnp.float32)
    squares = jnp.zeros((slots, lanes), jnp.float32)
    for j in range(blocks):
        part = wide[pl.ds(j, slots, stride=blocks), :]
        rows_ref[:, j * lanes : (j + 1) * lanes] = part.astype(jnp.bfloat16)
        total = total + part
        squares = squares + part * part
    sums_ref[:slots, :] = total
    sums_ref[slots:, :] = squares


def own_kernel(own_ref, up_hbm, rows_ref, sums_ref, up_ref, wide, sems):
    copies = start_all(((up_hbm, up_ref),), sems)
    unpack(own_ref, rows_ref, sums_ref, wide)
    copies[0].wait()


def give(part, wide, out_ref):
    slots = part.shape[0]
    blocks = part.shape[1] // lanes
    for j in range(blocks):
        wide[pl.ds(j, slots, stride=blocks), :] = part[:, j * lanes : (j + 1) * lanes]
    out_ref[...] = wide[...].astype(jnp.bfloat16)


def expert_kernel(rows_own, own_sums, other_ref, own_affine, other_affine, gate_ref, up_ref, down_hbm, hidden_ref, given_ref, down_kept, wide, rows_other, other_sums, down_given, sems):
    slots, width = rows_own.shape
    blocks = width // lanes
    half = lax.axis_index("tp")
    here = pl.multiple_of(half * width, width)
    there = pl.multiple_of((1 - half) * width, width)
    copies = start_all(
        (
            (down_hbm.at[0, :, pl.ds(there, width)], down_given),
            (down_hbm.at[0, :, pl.ds(here, width)], down_kept),
        ),
        sems,
    )
    unpack(other_ref, rows_other, other_sums, wide)
    sums = jnp.sum(own_sums[...] + other_sums[...], axis=1, keepdims=True)
    average = sums[:slots, :] / (2 * width)
    variance = sums[slots:, :] / (2 * width) - average * average
    inverse = jnp.broadcast_to(lax.rsqrt(variance + norm_eps), (slots, lanes))
    average = jnp.broadcast_to(average, (slots, lanes))

    def normalised(rows_ref, affine_ref):
        return jnp.concatenate(
            [
                (
                    (rows_ref[:, j * lanes : (j + 1) * lanes].astype(jnp.float32) - average)
                    * inverse
                    * affine_ref[j : j + 1, :]
                    + affine_ref[blocks + j : blocks + j + 1, :]
                ).astype(jnp.bfloat16)
                for j in range(blocks)
            ],
            axis=1,
        )

    own = normalised(rows_own, own_affine)
    other = normalised(rows_other, other_affine)

    def project(weight_ref):
        return jnp.dot(
            own, weight_ref[0, pl.ds(here, width), :], preferred_element_type=jnp.float32
        ) + jnp.dot(
            other, weight_ref[0, pl.ds(there, width), :], preferred_element_type=jnp.float32
        )

    gate_cut = jnp.minimum(project(gate_ref), clamp_limit)
    up_cut = jnp.clip(project(up_ref), -clamp_limit, clamp_limit)
    hidden = ((up_cut + 1.0) * gate_cut * jax.nn.sigmoid(sigmoid_slope * gate_cut)).astype(
        jnp.bfloat16
    )
    hidden_ref[...] = hidden
    copies[0].wait()
    give(jnp.dot(hidden, down_given[...], preferred_element_type=jnp.float32), wide, given_ref)
    copies[1].wait()


def kept_kernel(capacity, first_expert, hidden_ref, down_ref, routes_ref, logits_ref, pick_ref, kept_ref, high_ref, low_ref, wide):
    give(jnp.dot(hidden_ref[...], down_ref[...], preferred_element_type=jnp.float32), wide, kept_ref)
    top_count, rows = routes_ref.shape
    slots = pick_ref.shape[0]
    experts = slots // capacity
    exp_logits = jnp.exp(logits_ref[...])
    weights = exp_logits / jnp.sum(exp_logits, axis=0, keepdims=True)
    expert_id = expert_ids(experts, rows, first_expert)
    weight_of = jnp.zeros((experts, rows), jnp.float32)
    for k in range(top_count):
        weight_of = jnp.where(routes_ref[k : k + 1, :] == expert_id, weights[k : k + 1, :], weight_of)
    high = weight_of.astype(jnp.bfloat16)
    low = (weight_of - high.astype(jnp.float32)).astype(jnp.bfloat16)
    spread = spread_of(slots, experts, capacity)
    taken = pick_ref[...].astype(jnp.float32) > 0.0
    for part, part_ref in ((high, high_ref), (low, low_ref)):
        at_slots = jnp.dot(spread, part, preferred_element_type=jnp.float32)
        part_ref[...] = jnp.where(taken, at_slots, 0.0).astype(jnp.bfloat16)


def body(tokens, routes, gate_logits, norm_gain, norm_shift, gate_weight, up_weight, down_weight):
    experts = lax.axis_size("ep")
    rows, top_count = routes.shape
    width = tokens.shape[1]
    capacity = rows * top_count // experts + 2
    blocks = width // lanes
    slots = experts * capacity
    wire = (experts, capacity * blocks, lanes)
    tiles = (slots * blocks, lanes)
    bf16, f32 = jnp.bfloat16, jnp.float32
    vmem, hbm = pltpu.VMEM, pltpu.HBM

    packed, pick, affine, routes, gate_logits = in_kernel(
        "pack",
        functools.partial(pack_kernel, capacity, ring_order()[0]),
        [
            (tiles, bf16),
            ((slots, rows), bf16),
            ((2 * blocks, lanes), f32),
            ((top_count, rows), jnp.int32),
            ((top_count, rows), f32),
        ],
        scratch=[
            pltpu.VMEM(tokens.shape, bf16),
            pltpu.VMEM(tiles, f32),
            pltpu.SemaphoreType.DMA((5,)),
        ],
        kinds=[hbm] * 5,
    )(
        in_hbm(routes.T),
        in_hbm(gate_logits.T),
        in_hbm(tokens),
        in_hbm(norm_gain.reshape(blocks, lanes)),
        in_hbm(norm_shift.reshape(blocks, lanes)),
    )
    arrived = exchange(packed.reshape(wire)).reshape(tiles)
    arrived, affine = lax.optimization_barrier((arrived, affine))
    other = swap_tp(arrived)
    other_affine = swap_tp(affine)
    rows_own, own_sums, up_weight = in_kernel(
        "own",
        own_kernel,
        [((slots, width), bf16), ((2 * slots, lanes), f32), (up_weight.shape, bf16)],
        scratch=[pltpu.VMEM(tiles, f32), pltpu.SemaphoreType.DMA((1,))],
        kinds=[vmem, hbm],
    )(arrived, in_hbm(up_weight))
    down_half = (down_weight.shape[1], width)
    hidden, given, down_kept = in_kernel(
        "expert",
        expert_kernel,
        [((slots, gate_weight.shape[2]), bf16), (tiles, bf16), (down_half, bf16)],
        scratch=[
            pltpu.VMEM(tiles, f32),
            pltpu.VMEM((slots, width), bf16),
            pltpu.VMEM((2 * slots, lanes), f32),
            pltpu.VMEM(down_half, bf16),
            pltpu.SemaphoreType.DMA((2,)),
        ],
        kinds=[vmem] * 7 + [hbm],
    )(
        rows_own,
        own_sums,
        other,
        affine,
        other_affine,
        in_vmem(gate_weight),
        up_weight,
        in_hbm(down_weight),
    )
    kept, high, low = in_kernel(
        "kept",
        functools.partial(kept_kernel, capacity, ring_order()[0]),
        [(tiles, bf16), ((slots, rows), bf16), ((slots, rows), bf16)],
        scratch=[pltpu.VMEM(tiles, f32)],
        kinds=[vmem] * 5,
    )(hidden, down_kept, routes, gate_logits, pick)
    got = swap_tp(given)
    answered = (kept.astype(f32) + got.astype(f32)).astype(bf16)
    returned = exchange(answered.reshape(wire)).reshape(slots, width)

    def blended(blend):
        return lax.dot_general(
            blend, returned, (((0,), (0,)), ((), ())), preferred_element_type=f32
        )

    return (blended(high) + blended(low)).astype(bf16)


def solution(mesh):
    placed = (
        P(("grp", "ep"), "tp"),
        P(("grp", "ep"), None),
        P(("grp", "ep"), None),
        P("tp"),
        P("tp"),
        P("ep", None, "tp"),
        P("ep", None, "tp"),
        P("ep", "tp", None),
    )
    return jax.shard_map(
        body, mesh=mesh, in_specs=placed, out_specs=P(("grp", "ep"), "tp"), check_vma=False
    )
```

```python
import functools

import jax
import jax.numpy as jnp
from jax import lax
from jax.experimental import pallas as pl
from jax.experimental.pallas import tpu as pltpu
from jax.sharding import PartitionSpec as P

norm_eps = 1e-05
clamp_limit = 7.0
sigmoid_slope = 1.702
lanes = 128


def swap_tp(x):
    return lax.ppermute(x, "tp", [(0, 1), (1, 0)])


def ring_order():
    count = lax.axis_size("ep")
    return [(3 * count // 4 + k) % count for k in range(count)]


def exchange(x):
    return lax.all_to_all(
        x, "ep", split_axis=0, concat_axis=0, axis_index_groups=[ring_order()], tiled=True
    )


def in_kernel(name, kernel, outs, scratch, kinds):
    vmem = pl.BlockSpec(memory_space=pltpu.VMEM)
    return pl.pallas_call(
        kernel,
        out_shape=tuple(jax.ShapeDtypeStruct(shape, dtype) for shape, dtype in outs),
        in_specs=[pl.BlockSpec(memory_space=kind) for kind in kinds],
        out_specs=tuple(vmem for _ in outs),
        scratch_shapes=list(scratch),
        compiler_params=pltpu.CompilerParams(vmem_limit_bytes=16 << 20),
        name=name,
    )


def in_vmem(x):
    return pltpu.with_memory_space_constraint(x, pltpu.VMEM)


def in_hbm(x):
    return pltpu.with_memory_space_constraint(x, pltpu.HBM)


def start_all(pairs, sems):
    copies = [pltpu.make_async_copy(*pair, sems.at[i]) for i, pair in enumerate(pairs)]
    for copy in copies:
        copy.start()
    return copies


def expert_ids(experts, rows, first_expert):
    return (lax.broadcasted_iota(jnp.int32, (experts, rows), 0) + first_expert) % experts


def spread_of(slots, experts, capacity):
    slot_id = lax.broadcasted_iota(jnp.int32, (slots, experts), 0)
    first = lax.broadcasted_iota(jnp.int32, (slots, experts), 1) * capacity
    return jnp.where((slot_id >= first) & (slot_id < first + capacity), 1.0, 0.0).astype(
        jnp.bfloat16
    )


def pack_kernel(capacity, first_expert, routes_hbm, logits_hbm, tokens_hbm, gain_hbm, shift_hbm, packed_ref, pick_ref, affine_ref, routes_ref, logits_ref, tokens_ref, wide, sems):
    top_count, rows = routes_ref.shape
    slots = pick_ref.shape[0]
    experts = slots // capacity
    blocks = tokens_ref.shape[1] // lanes
    copies = start_all(
        (
            (routes_hbm, routes_ref),
            (logits_hbm, logits_ref),
            (tokens_hbm, tokens_ref),
            (gain_hbm, affine_ref.at[0:blocks]),
            (shift_hbm, affine_ref.at[blocks : 2 * blocks]),
        ),
        sems,
    )
    copies[0].wait()
    expert_id = expert_ids(experts, rows, first_expert)
    place = lax.broadcasted_iota(jnp.int32, (experts, rows), 0) * capacity
    matches = [routes_ref[k : k + 1, :] == expert_id for k in range(top_count)]
    chosen = functools.reduce(jnp.logical_or, matches)
    earlier = lax.broadcasted_iota(jnp.int32, (rows, rows), 0) < lax.broadcasted_iota(
        jnp.int32, (rows, rows), 1
    )
    rank = jnp.dot(
        jnp.where(chosen, 1.0, 0.0).astype(jnp.bfloat16),
        jnp.where(earlier, 1.0, 0.0).astype(jnp.bfloat16),
        preferred_element_type=jnp.float32,
    )
    slot_of = jnp.where(
        chosen, rank + place.astype(jnp.float32), -1.0
    ).astype(jnp.bfloat16)
    spread = spread_of(slots, experts, capacity)
    at_slots = jnp.dot(spread, slot_of, preferred_element_type=jnp.float32)
    taken = at_slots == lax.broadcasted_iota(jnp.int32, (slots, rows), 0).astype(jnp.float32)
    pick = jnp.where(taken, 1.0, 0.0).astype(jnp.bfloat16)
    pick_ref[...] = pick
    copies[2].wait()
    packed = jnp.dot(pick, tokens_ref[...], preferred_element_type=jnp.float32)
    for j in range(blocks):
        wide[pl.ds(j, slots, stride=blocks), :] = packed[:, j * lanes : (j + 1) * lanes]
    packed_ref[...] = wide[...].astype(jnp.bfloat16)
    copies[1].wait()
    for copy in copies[3:]:
        copy.wait()


def unpack(tiles_ref, rows_ref, sums_ref, wide):
    slots, width = rows_ref.shape
    blocks = width // lanes
    wide[...] = tiles_ref[...].astype(jnp.float32)
    total = jnp.zeros((slots, lanes), jnp.float32)
    squares = jnp.zeros((slots, lanes), jnp.float32)
    for j in range(blocks):
        part = wide[pl.ds(j, slots, stride=blocks), :]
        rows_ref[:, j * lanes : (j + 1) * lanes] = part.astype(jnp.bfloat16)
        total = total + part
        squares = squares + part * part
    sums_ref[:slots, :] = total
    sums_ref[slots:, :] = squares


def own_kernel(own_ref, up_hbm, rows_ref, sums_ref, up_ref, wide, sems):
    width = rows_ref.shape[1]
    here = pl.multiple_of(lax.axis_index("tp") * width, width)
    copies = start_all(((up_hbm.at[0, pl.ds(here, width), :], up_ref),), sems)
    unpack(own_ref, rows_ref, sums_ref, wide)
    copies[0].wait()


def give(part, wide, out_ref):
    slots = part.shape[0]
    blocks = part.shape[1] // lanes
    for j in range(blocks):
        wide[pl.ds(j, slots, stride=blocks), :] = part[:, j * lanes : (j + 1) * lanes]
    out_ref[...] = wide[...].astype(jnp.bfloat16)


def expert_kernel(rows_own, own_sums, other_ref, own_affine, other_affine, gate_ref, up_own, up_hbm, down_hbm, hidden_ref, given_ref, down_kept, wide, rows_other, other_sums, up_other, down_given, sems):
    slots, width = rows_own.shape
    blocks = width // lanes
    half = lax.axis_index("tp")
    here = pl.multiple_of(half * width, width)
    there = pl.multiple_of((1 - half) * width, width)
    copies = start_all(
        (
            (up_hbm.at[0, pl.ds(there, width), :], up_other),
            (down_hbm.at[0, :, pl.ds(there, width)], down_given),
            (down_hbm.at[0, :, pl.ds(here, width)], down_kept),
        ),
        sems,
    )
    unpack(other_ref, rows_other, other_sums, wide)
    sums = jnp.sum(own_sums[...] + other_sums[...], axis=1, keepdims=True)
    average = sums[:slots, :] / (2 * width)
    variance = sums[slots:, :] / (2 * width) - average * average
    inverse = jnp.broadcast_to(lax.rsqrt(variance + norm_eps), (slots, lanes))
    average = jnp.broadcast_to(average, (slots, lanes))

    def normalised(rows_ref, affine_ref):
        return jnp.concatenate(
            [
                (
                    (rows_ref[:, j * lanes : (j + 1) * lanes].astype(jnp.float32) - average)
                    * inverse
                    * affine_ref[j : j + 1, :]
                    + affine_ref[blocks + j : blocks + j + 1, :]
                ).astype(jnp.bfloat16)
                for j in range(blocks)
            ],
            axis=1,
        )

    own = normalised(rows_own, own_affine)
    other = normalised(rows_other, other_affine)

    def project(own_weight, other_weight):
        return jnp.dot(own, own_weight, preferred_element_type=jnp.float32) + jnp.dot(
            other, other_weight, preferred_element_type=jnp.float32
        )

    gate_pre = project(gate_ref[0, pl.ds(here, width), :], gate_ref[0, pl.ds(there, width), :])
    gate_cut = jnp.minimum(gate_pre, clamp_limit)
    copies[0].wait()
    up_cut = jnp.clip(project(up_own[...], up_other[...]), -clamp_limit, clamp_limit)
    hidden = ((up_cut + 1.0) * gate_cut * jax.nn.sigmoid(sigmoid_slope * gate_cut)).astype(
        jnp.bfloat16
    )
    hidden_ref[...] = hidden
    copies[1].wait()
    give(jnp.dot(hidden, down_given[...], preferred_element_type=jnp.float32), wide, given_ref)
    copies[2].wait()


def kept_kernel(capacity, first_expert, hidden_ref, down_ref, routes_ref, logits_ref, pick_ref, kept_ref, high_ref, low_ref, wide):
    give(jnp.dot(hidden_ref[...], down_ref[...], preferred_element_type=jnp.float32), wide, kept_ref)
    top_count, rows = routes_ref.shape
    slots = pick_ref.shape[0]
    experts = slots // capacity
    exp_logits = jnp.exp(logits_ref[...])
    weights = exp_logits / jnp.sum(exp_logits, axis=0, keepdims=True)
    expert_id = expert_ids(experts, rows, first_expert)
    weight_of = jnp.zeros((experts, rows), jnp.float32)
    for k in range(top_count):
        weight_of = jnp.where(routes_ref[k : k + 1, :] == expert_id, weights[k : k + 1, :], weight_of)
    high = weight_of.astype(jnp.bfloat16)
    low = (weight_of - high.astype(jnp.float32)).astype(jnp.bfloat16)
    spread = spread_of(slots, experts, capacity)
    taken = pick_ref[...].astype(jnp.float32) > 0.0
    for part, part_ref in ((high, high_ref), (low, low_ref)):
        at_slots = jnp.dot(spread, part, preferred_element_type=jnp.float32)
        part_ref[...] = jnp.where(taken, at_slots, 0.0).astype(jnp.bfloat16)


def body(tokens, routes, gate_logits, norm_gain, norm_shift, gate_weight, up_weight, down_weight):
    experts = lax.axis_size("ep")
    rows, top_count = routes.shape
    width = tokens.shape[1]
    capacity = rows * top_count // experts + 2
    blocks = width // lanes
    slots = experts * capacity
    wire = (experts, capacity * blocks, lanes)
    tiles = (slots * blocks, lanes)
    bf16, f32 = jnp.bfloat16, jnp.float32
    vmem, hbm = pltpu.VMEM, pltpu.HBM

    packed, pick, affine, routes, gate_logits = in_kernel(
        "pack",
        functools.partial(pack_kernel, capacity, ring_order()[0]),
        [
            (tiles, bf16),
            ((slots, rows), bf16),
            ((2 * blocks, lanes), f32),
            ((top_count, rows), jnp.int32),
            ((top_count, rows), f32),
        ],
        scratch=[
            pltpu.VMEM(tokens.shape, bf16),
            pltpu.VMEM(tiles, f32),
            pltpu.SemaphoreType.DMA((5,)),
        ],
        kinds=[hbm] * 5,
    )(
        in_hbm(routes.T),
        in_hbm(gate_logits.T),
        in_hbm(tokens),
        in_hbm(norm_gain.reshape(blocks, lanes)),
        in_hbm(norm_shift.reshape(blocks, lanes)),
    )
    arrived = exchange(packed.reshape(wire)).reshape(tiles)
    arrived, affine = lax.optimization_barrier((arrived, affine))
    other = swap_tp(arrived)
    other_affine = swap_tp(affine)
    up_half = (width, up_weight.shape[2])
    rows_own, own_sums, up_own = in_kernel(
        "own",
        own_kernel,
        [((slots, width), bf16), ((2 * slots, lanes), f32), (up_half, bf16)],
        scratch=[pltpu.VMEM(tiles, f32), pltpu.SemaphoreType.DMA((1,))],
        kinds=[vmem, hbm],
    )(arrived, in_hbm(up_weight))
    down_half = (down_weight.shape[1], width)
    hidden, given, down_kept = in_kernel(
        "expert",
        expert_kernel,
        [((slots, gate_weight.shape[2]), bf16), (tiles, bf16), (down_half, bf16)],
        scratch=[
            pltpu.VMEM(tiles, f32),
            pltpu.VMEM((slots, width), bf16),
            pltpu.VMEM((2 * slots, lanes), f32),
            pltpu.VMEM(up_half, bf16),
            pltpu.VMEM(down_half, bf16),
            pltpu.SemaphoreType.DMA((3,)),
        ],
        kinds=[vmem] * 7 + [hbm] * 2,
    )(
        rows_own,
        own_sums,
        other,
        affine,
        other_affine,
        in_vmem(gate_weight),
        up_own,
        in_hbm(up_weight),
        in_hbm(down_weight),
    )
    kept, high, low = in_kernel(
        "kept",
        functools.partial(kept_kernel, capacity, ring_order()[0]),
        [(tiles, bf16), ((slots, rows), bf16), ((slots, rows), bf16)],
        scratch=[pltpu.VMEM(tiles, f32)],
        kinds=[vmem] * 5,
    )(hidden, down_kept, routes, gate_logits, pick)
    got = swap_tp(given)
    answered = (kept.astype(f32) + got.astype(f32)).astype(bf16)
    returned = exchange(answered.reshape(wire)).reshape(slots, width)

    def blended(blend):
        return lax.dot_general(
            blend, returned, (((0,), (0,)), ((), ())), preferred_element_type=f32
        )

    return (blended(high) + blended(low)).astype(bf16)


def solution(mesh):
    placed = (
        P(("grp", "ep"), "tp"),
        P(("grp", "ep"), None),
        P(("grp", "ep"), None),
        P("tp"),
        P("tp"),
        P("ep", None, "tp"),
        P("ep", None, "tp"),
        P("ep", "tp", None),
    )
    return jax.shard_map(
        body, mesh=mesh, in_specs=placed, out_specs=P(("grp", "ep"), "tp"), check_vma=False
    )
```

```python
import functools

import jax
import jax.numpy as jnp
from jax import lax
from jax.experimental import pallas as pl
from jax.experimental.pallas import tpu as pltpu
from jax.sharding import PartitionSpec as P

norm_eps = 1e-05
clamp_limit = 7.0
sigmoid_slope = 1.702
lanes = 128


def swap_tp(x):
    return lax.ppermute(x, "tp", [(0, 1), (1, 0)])


def ring_order():
    count = lax.axis_size("ep")
    return [(5 * count // 8 + k) % count for k in range(count)]


def exchange(x):
    return lax.all_to_all(
        x, "ep", split_axis=0, concat_axis=0, axis_index_groups=[ring_order()], tiled=True
    )


def in_kernel(name, kernel, outs, scratch, kinds):
    vmem = pl.BlockSpec(memory_space=pltpu.VMEM)
    return pl.pallas_call(
        kernel,
        out_shape=tuple(jax.ShapeDtypeStruct(shape, dtype) for shape, dtype in outs),
        in_specs=[pl.BlockSpec(memory_space=kind) for kind in kinds],
        out_specs=tuple(vmem for _ in outs),
        scratch_shapes=list(scratch),
        compiler_params=pltpu.CompilerParams(vmem_limit_bytes=16 << 20),
        name=name,
    )


def in_vmem(x):
    return pltpu.with_memory_space_constraint(x, pltpu.VMEM)


def in_hbm(x):
    return pltpu.with_memory_space_constraint(x, pltpu.HBM)


def start_all(pairs, sems):
    copies = [pltpu.make_async_copy(*pair, sems.at[i]) for i, pair in enumerate(pairs)]
    for copy in copies:
        copy.start()
    return copies


def expert_ids(experts, rows, first_expert):
    return (lax.broadcasted_iota(jnp.int32, (experts, rows), 0) + first_expert) % experts


def spread_of(slots, experts, capacity):
    slot_id = lax.broadcasted_iota(jnp.int32, (slots, experts), 0)
    first = lax.broadcasted_iota(jnp.int32, (slots, experts), 1) * capacity
    return jnp.where((slot_id >= first) & (slot_id < first + capacity), 1.0, 0.0).astype(
        jnp.bfloat16
    )


def pack_kernel(capacity, first_expert, routes_hbm, logits_hbm, tokens_hbm, gain_hbm, shift_hbm, packed_ref, pick_ref, affine_ref, routes_ref, logits_ref, tokens_ref, wide, sems):
    top_count, rows = routes_ref.shape
    slots = pick_ref.shape[0]
    experts = slots // capacity
    blocks = tokens_ref.shape[1] // lanes
    copies = start_all(
        (
            (routes_hbm, routes_ref),
            (logits_hbm, logits_ref),
            (tokens_hbm, tokens_ref),
            (gain_hbm, affine_ref.at[0:blocks]),
            (shift_hbm, affine_ref.at[blocks : 2 * blocks]),
        ),
        sems,
    )
    copies[0].wait()
    expert_id = expert_ids(experts, rows, first_expert)
    place = lax.broadcasted_iota(jnp.int32, (experts, rows), 0) * capacity
    matches = [routes_ref[k : k + 1, :] == expert_id for k in range(top_count)]
    chosen = functools.reduce(jnp.logical_or, matches)
    earlier = lax.broadcasted_iota(jnp.int32, (rows, rows), 0) < lax.broadcasted_iota(
        jnp.int32, (rows, rows), 1
    )
    rank = jnp.dot(
        jnp.where(chosen, 1.0, 0.0).astype(jnp.bfloat16),
        jnp.where(earlier, 1.0, 0.0).astype(jnp.bfloat16),
        preferred_element_type=jnp.float32,
    )
    slot_of = jnp.where(
        chosen, rank + place.astype(jnp.float32), -1.0
    ).astype(jnp.bfloat16)
    spread = spread_of(slots, experts, capacity)
    at_slots = jnp.dot(spread, slot_of, preferred_element_type=jnp.float32)
    taken = at_slots == lax.broadcasted_iota(jnp.int32, (slots, rows), 0).astype(jnp.float32)
    pick = jnp.where(taken, 1.0, 0.0).astype(jnp.bfloat16)
    pick_ref[...] = pick
    copies[2].wait()
    packed = jnp.dot(pick, tokens_ref[...], preferred_element_type=jnp.float32)
    for j in range(blocks):
        wide[pl.ds(j, slots, stride=blocks), :] = packed[:, j * lanes : (j + 1) * lanes]
    packed_ref[...] = wide[...].astype(jnp.bfloat16)
    copies[1].wait()
    for copy in copies[3:]:
        copy.wait()


def unpack(tiles_ref, rows_ref, sums_ref, wide):
    slots, width = rows_ref.shape
    blocks = width // lanes
    wide[...] = tiles_ref[...].astype(jnp.float32)
    total = jnp.zeros((slots, lanes), jnp.float32)
    squares = jnp.zeros((slots, lanes), jnp.float32)
    for j in range(blocks):
        part = wide[pl.ds(j, slots, stride=blocks), :]
        rows_ref[:, j * lanes : (j + 1) * lanes] = part.astype(jnp.bfloat16)
        total = total + part
        squares = squares + part * part
    sums_ref[:slots, :] = total
    sums_ref[slots:, :] = squares


def own_kernel(own_ref, up_hbm, rows_ref, sums_ref, up_ref, wide, sems):
    copies = start_all(((up_hbm, up_ref),), sems)
    unpack(own_ref, rows_ref, sums_ref, wide)
    copies[0].wait()


def give(part, wide, out_ref):
    slots = part.shape[0]
    blocks = part.shape[1] // lanes
    for j in range(blocks):
        wide[pl.ds(j, slots, stride=blocks), :] = part[:, j * lanes : (j + 1) * lanes]
    out_ref[...] = wide[...].astype(jnp.bfloat16)


def expert_kernel(rows_own, own_sums, other_ref, own_affine, other_affine, gate_ref, up_ref, down_hbm, hidden_ref, given_ref, down_kept, wide, rows_other, other_sums, down_given, sems):
    slots, width = rows_own.shape
    blocks = width // lanes
    half = lax.axis_index("tp")
    here = pl.multiple_of(half * width, width)
    there = pl.multiple_of((1 - half) * width, width)
    copies = start_all(
        (
            (down_hbm.at[0, :, pl.ds(there, width)], down_given),
            (down_hbm.at[0, :, pl.ds(here, width)], down_kept),
        ),
        sems,
    )
    unpack(other_ref, rows_other, other_sums, wide)
    sums = jnp.sum(own_sums[...] + other_sums[...], axis=1, keepdims=True)
    average = sums[:slots, :] / (2 * width)
    variance = sums[slots:, :] / (2 * width) - average * average
    inverse = jnp.broadcast_to(lax.rsqrt(variance + norm_eps), (slots, lanes))
    average = jnp.broadcast_to(average, (slots, lanes))

    def normalised(rows_ref, affine_ref):
        return jnp.concatenate(
            [
                (
                    (rows_ref[:, j * lanes : (j + 1) * lanes].astype(jnp.float32) - average)
                    * inverse
                    * affine_ref[j : j + 1, :]
                    + affine_ref[blocks + j : blocks + j + 1, :]
                ).astype(jnp.bfloat16)
                for j in range(blocks)
            ],
            axis=1,
        )

    own = normalised(rows_own, own_affine)
    other = normalised(rows_other, other_affine)

    def project(weight_ref):
        return jnp.dot(
            own, weight_ref[0, pl.ds(here, width), :], preferred_element_type=jnp.float32
        ) + jnp.dot(
            other, weight_ref[0, pl.ds(there, width), :], preferred_element_type=jnp.float32
        )

    gate_cut = jnp.minimum(project(gate_ref), clamp_limit)
    up_cut = jnp.clip(project(up_ref), -clamp_limit, clamp_limit)
    hidden = ((up_cut + 1.0) * gate_cut * jax.nn.sigmoid(sigmoid_slope * gate_cut)).astype(
        jnp.bfloat16
    )
    hidden_ref[...] = hidden
    copies[0].wait()
    give(jnp.dot(hidden, down_given[...], preferred_element_type=jnp.float32), wide, given_ref)
    copies[1].wait()


def kept_kernel(capacity, first_expert, hidden_ref, down_ref, routes_ref, logits_ref, pick_ref, kept_ref, high_ref, low_ref, wide):
    give(jnp.dot(hidden_ref[...], down_ref[...], preferred_element_type=jnp.float32), wide, kept_ref)
    top_count, rows = routes_ref.shape
    slots = pick_ref.shape[0]
    experts = slots // capacity
    exp_logits = jnp.exp(logits_ref[...])
    weights = exp_logits / jnp.sum(exp_logits, axis=0, keepdims=True)
    expert_id = expert_ids(experts, rows, first_expert)
    weight_of = jnp.zeros((experts, rows), jnp.float32)
    for k in range(top_count):
        weight_of = jnp.where(routes_ref[k : k + 1, :] == expert_id, weights[k : k + 1, :], weight_of)
    high = weight_of.astype(jnp.bfloat16)
    low = (weight_of - high.astype(jnp.float32)).astype(jnp.bfloat16)
    spread = spread_of(slots, experts, capacity)
    taken = pick_ref[...].astype(jnp.float32) > 0.0
    for part, part_ref in ((high, high_ref), (low, low_ref)):
        at_slots = jnp.dot(spread, part, preferred_element_type=jnp.float32)
        part_ref[...] = jnp.where(taken, at_slots, 0.0).astype(jnp.bfloat16)


def body(tokens, routes, gate_logits, norm_gain, norm_shift, gate_weight, up_weight, down_weight):
    experts = lax.axis_size("ep")
    rows, top_count = routes.shape
    width = tokens.shape[1]
    capacity = rows * top_count // experts + 2
    blocks = width // lanes
    slots = experts * capacity
    wire = (experts, capacity * blocks, lanes)
    tiles = (slots * blocks, lanes)
    bf16, f32 = jnp.bfloat16, jnp.float32
    vmem, hbm = pltpu.VMEM, pltpu.HBM

    packed, pick, affine, routes, gate_logits = in_kernel(
        "pack",
        functools.partial(pack_kernel, capacity, ring_order()[0]),
        [
            (tiles, bf16),
            ((slots, rows), bf16),
            ((2 * blocks, lanes), f32),
            ((top_count, rows), jnp.int32),
            ((top_count, rows), f32),
        ],
        scratch=[
            pltpu.VMEM(tokens.shape, bf16),
            pltpu.VMEM(tiles, f32),
            pltpu.SemaphoreType.DMA((5,)),
        ],
        kinds=[hbm] * 5,
    )(
        in_hbm(routes.T),
        in_hbm(gate_logits.T),
        in_hbm(tokens),
        in_hbm(norm_gain.reshape(blocks, lanes)),
        in_hbm(norm_shift.reshape(blocks, lanes)),
    )
    arrived = exchange(packed.reshape(wire)).reshape(tiles)
    arrived, affine = lax.optimization_barrier((arrived, affine))
    other = swap_tp(arrived)
    other_affine = swap_tp(affine)
    rows_own, own_sums, up_weight = in_kernel(
        "own",
        own_kernel,
        [((slots, width), bf16), ((2 * slots, lanes), f32), (up_weight.shape, bf16)],
        scratch=[pltpu.VMEM(tiles, f32), pltpu.SemaphoreType.DMA((1,))],
        kinds=[vmem, hbm],
    )(arrived, in_hbm(up_weight))
    down_half = (down_weight.shape[1], width)
    hidden, given, down_kept = in_kernel(
        "expert",
        expert_kernel,
        [((slots, gate_weight.shape[2]), bf16), (tiles, bf16), (down_half, bf16)],
        scratch=[
            pltpu.VMEM(tiles, f32),
            pltpu.VMEM((slots, width), bf16),
            pltpu.VMEM((2 * slots, lanes), f32),
            pltpu.VMEM(down_half, bf16),
            pltpu.SemaphoreType.DMA((2,)),
        ],
        kinds=[vmem] * 7 + [hbm],
    )(
        rows_own,
        own_sums,
        other,
        affine,
        other_affine,
        in_vmem(gate_weight),
        up_weight,
        in_hbm(down_weight),
    )
    kept, high, low = in_kernel(
        "kept",
        functools.partial(kept_kernel, capacity, ring_order()[0]),
        [(tiles, bf16), ((slots, rows), bf16), ((slots, rows), bf16)],
        scratch=[pltpu.VMEM(tiles, f32)],
        kinds=[vmem] * 5,
    )(hidden, down_kept, routes, gate_logits, pick)
    got = swap_tp(given)
    answered = (kept.astype(f32) + got.astype(f32)).astype(bf16)
    returned = exchange(answered.reshape(wire)).reshape(slots, width)

    def blended(blend):
        return lax.dot_general(
            blend, returned, (((0,), (0,)), ((), ())), preferred_element_type=f32
        )

    return (blended(high) + blended(low)).astype(bf16)


def solution(mesh):
    placed = (
        P(("grp", "ep"), "tp"),
        P(("grp", "ep"), None),
        P(("grp", "ep"), None),
        P("tp"),
        P("tp"),
        P("ep", None, "tp"),
        P("ep", None, "tp"),
        P("ep", "tp", None),
    )
    return jax.shard_map(
        body, mesh=mesh, in_specs=placed, out_specs=P(("grp", "ep"), "tp"), check_vma=False
    )
```
